256 devices in a mesh: ep: 128 (over z, y, x), tp: 2 (over core).
Axes of the slice: x: 4, y: 4, z: 8, core: 2. Of those that a mesh axis runs over, the one named last changes fastest.
Arguments:
- tokens: bfloat16 [8192, 1024], P('ep', 'tp'), may hold values from -6 to 6
- norm_gain: float32 [1024], P('tp'), may hold values from 0.1 to 1.9
- routing: int32 [8192, 2], P('ep'), may hold values from 0 to 255, as said below
- route_weight: float32 [8192, 2], P('ep'), may hold values from 0.25 to 1
- w_gate: bfloat16 [256, 1024, 512], P('ep', None, 'tp'), may hold values from -0.1875 to 0.1875
- w_up: bfloat16 [256, 1024, 512], P('ep', None, 'tp'), may hold values from -0.1875 to 0.1875
- w_down: bfloat16 [256, 512, 1024], P('ep', None, 'tp'), may hold values from -0.25 to 0.25
Outputs:
- mixed: bfloat16 [8192, 1024], P('ep', 'tp')
The draws below stay inside these ranges and needn't reach their ends.
Inputs may be any that keep to these rules, and one draw needn't show every extreme that they name: `routing`: each row names 2 different experts, all in the same group of 8 consecutive expert numbers. Among the rows of one device (aligned blocks of 64 rows) no expert is named more than 8 times, and in every block some expert is named exactly 8 times.
All inputs are finite; a program needn't handle non-finite values.
Results may differ from the reference program's by a relative error of at most 0.0015.
Values may be sent and summed in bfloat16 or wider, within the bound.
A program may use at most 64 MiB of HBM per device.

```python
import jax
import jax.numpy as jnp
from jax import lax

D = 1024
FFE = 512
TOP_K = 2
GROUP_EXP = 8
EXP_DEV = 2
CAP = 8
TOK_DEV = 64
EXPERTS = 256
TOKENS = 8192


def route_table(key):
    blocks = TOKENS // TOK_DEV
    groups = EXPERTS // GROUP_EXP
    semi_cluster = GROUP_EXP // 2
    opening_tally = EXPERTS // 2
    cell_count = TOK_DEV // CAP
    pop_key = jax.random.fold_in(key, 11)
    group_scores = jax.random.randint(pop_key, (groups,), 0, 1 << 20) * groups + jnp.arange(groups)
    ranking = jnp.argsort(jnp.argsort(group_scores))
    favoured_specialist = ranking < max(1, groups // 4)
    extra_cluster = jnp.where(favoured_specialist, 400, 0)
    base_key = jax.random.fold_in(key, 23)

    def one_block(block_id):
        block_key = jax.random.fold_in(base_key, block_id)
        perm_key, rating_seed, seat_key, flip_key = jax.random.split(block_key, 4)
        raw = jax.random.randint(perm_key, (groups, GROUP_EXP), 0, 1 << 20) * GROUP_EXP + jnp.arange(GROUP_EXP)[None, :]
        local_perm = jnp.argsort(raw, axis=1)
        pair_table = (jnp.arange(groups)[:, None] * GROUP_EXP + local_perm).reshape(opening_tally, 2)
        position = jnp.argsort(pair_table.reshape(-1))
        slot_of = position // 2
        forward = (block_id + blocks // 2) % blocks * EXP_DEV
        previous = (block_id + blocks - 1) % blocks * EXP_DEV
        opening_labels = jnp.arange(opening_tally)
        affinity_grades = jax.random.randint(rating_seed, (opening_tally,), 0, 1024) + extra_cluster[opening_labels // semi_cluster]
        affinity_grades = affinity_grades + 8192 * (opening_labels == slot_of[forward]) + 8192 * (opening_labels == slot_of[previous])
        affinity_grades = affinity_grades * opening_tally + opening_labels
        unused, chosen = lax.top_k(affinity_grades, cell_count)
        seating = jax.random.permutation(seat_key, TOK_DEV)
        cell_of = seating // CAP
        pair_ids = pair_table[chosen[cell_of]]
        flipped = jax.random.randint(flip_key, (TOK_DEV,), 0, 2)
        first_pick = jnp.where(flipped == 1, pair_ids[:, 1], pair_ids[:, 0])
        second_pick = jnp.where(flipped == 1, pair_ids[:, 0], pair_ids[:, 1])
        return jnp.stack([first_pick, second_pick], axis=1)
    table = jax.vmap(one_block)(jnp.arange(blocks))
    return table.reshape(TOKENS, 2)


def draw_routing(key, part):
    return route_table(key).astype(jnp.int32)


def block_levels(key, shape, pieces, low, top_value):
    loudness, own = 1.0, jax.random.fold_in(key, 6)
    for dim, blocks in pieces:
        steps = jnp.exp(jax.random.uniform(jax.random.fold_in(own, dim), (blocks,), jnp.float32, low / len(pieces), top_value / len(pieces)))
        loudness = loudness * jnp.repeat(steps, shape[dim] // blocks).reshape([-1 if axis == dim else 1 for axis in range(len(shape))])
    return loudness


def scatter_about(stream_key, extent, width, reach, pieces=(), kind=jnp.bfloat16):
    loudness = block_levels(stream_key, extent, pieces, -0.22, 0.18) if pieces else 1.0
    array = jax.random.normal(stream_key, extent, jnp.float32) * width * loudness
    return jnp.minimum(jnp.maximum(array, -reach), reach).astype(kind)


def setup_inputs(seed: int = 0) -> dict:
    key_of = jax.random.split(jax.random.key(seed), 8)
    return {
        "tokens": scatter_about(key_of[0], (TOKENS, D), 1.0, 6.0, ((0, 128), (1, 2))),
        "norm_gain": jnp.clip(1.0 + 0.18 * jax.random.normal(key_of[1], (D,), jnp.float32), 0.1, 1.9),
        "routing": draw_routing(jax.random.fold_in(key_of[7], 71), 0),
        "route_weight": jnp.clip(0.25 + 0.75 * jax.random.uniform(key_of[3], (TOKENS, TOP_K), jnp.float32) ** block_levels(key_of[3], (TOKENS, TOP_K), ((0, 128),), -0.2, 0.2), 0.25, 1.0),
        "w_gate": scatter_about(key_of[4], (EXPERTS, D, FFE), D ** -0.5, 0.1875, ((0, 128), (2, 2))),
        "w_up": scatter_about(key_of[5], (EXPERTS, D, FFE), D ** -0.5, 0.1875, ((0, 128), (2, 2))),
        "w_down": scatter_about(key_of[6], (EXPERTS, FFE, D), FFE ** -0.5, 0.25, ((0, 128), (2, 2))),
    }


epsilon = 1e-06

def reference(tokens, norm_gain, routing, route_weight, w_gate, w_up, w_down):
    row_span = 32
    float_rows = tokens.astype(jnp.float32)
    scale = lax.rsqrt(lax.optimization_barrier(jnp.mean(float_rows * float_rows, axis=1, keepdims=True)) + epsilon)
    normed = (float_rows * scale * norm_gain[None, :]).astype(jnp.bfloat16)
    count = TOKENS * TOP_K
    flat_expert = routing.reshape(-1).astype(jnp.int32)
    flat_token = (jnp.arange(count) // TOP_K).astype(jnp.int32)
    flat_weight = route_weight.reshape(-1)
    sorting = jnp.argsort(flat_expert, stable=True).astype(jnp.int32)
    sorted_expert = flat_expert[sorting]
    counts = jnp.zeros((EXPERTS,), jnp.int32).at[flat_expert].add(1)
    starts = (jnp.cumsum(counts) - counts).astype(jnp.int32)
    padded = ((counts + row_span - 1) // row_span * row_span).astype(jnp.int32)
    pad_end = jnp.cumsum(padded).astype(jnp.int32)
    pad_start = (pad_end - padded).astype(jnp.int32)
    target = (pad_start[sorted_expert] + jnp.arange(count).astype(jnp.int32) - starts[sorted_expert]).astype(jnp.int32)
    block_count = -(-count // row_span) + EXPERTS
    row_total = block_count * row_span
    buffer = jnp.zeros((row_total, D), jnp.bfloat16).at[target].set(normed[flat_token[sorting]])
    block_expert = jnp.searchsorted(pad_end, (jnp.arange(block_count) * row_span).astype(jnp.int32), side='right')
    block_expert = jnp.minimum(block_expert.astype(jnp.int32), EXPERTS - 1).astype(jnp.int32)

    def run_block(inputs):
        block_rows, expert = inputs
        gate_acc = jnp.dot(block_rows, w_gate[expert], preferred_element_type=jnp.float32)
        up_acc = jnp.dot(block_rows, w_up[expert], preferred_element_type=jnp.float32)
        hidden = (jax.nn.silu(gate_acc) * up_acc).astype(jnp.bfloat16)
        return jnp.dot(hidden, w_down[expert], preferred_element_type=jnp.float32).astype(jnp.bfloat16)
    result = lax.map(run_block, (buffer.reshape(block_count, row_span, D), block_expert)).reshape(row_total, D)
    picked = result[target].astype(jnp.float32) * flat_weight[sorting][:, None]
    combined = jax.ops.segment_sum(picked, flat_token[sorting], num_segments=TOKENS)
    return combined.astype(jnp.bfloat16)
```

```python
import jax
import jax.numpy as jnp
from jax import lax
from jax.experimental import pallas as pl
from jax.experimental.pallas import tpu as pltpu
from jax.sharding import PartitionSpec as P

F32 = jnp.float32
BF16 = jnp.bfloat16
EPS = 1e-06

X, Y, Z = 4, 4, 8
TOK = 64
HALF = 512
FULL = 1024
HID = 256
SLOTS = 8
BATCHES = 8
ROWS = 256
PACK = 32
LAST = BATCHES - 1

NT = (((1,), (1,)), ((), ()))


def dot(a, b):
    return jnp.dot(a, b, preferred_element_type=F32)


def iota(shape, dim):
    return lax.broadcasted_iota(jnp.int32, shape, dim)


def rem(a, n):
    return lax.rem(a, jnp.int32(n))


def kernel(
    tok, gain, picks, pick_w, wg_hbm, wu_hbm, wd_hbm, out,
    wg, wu, wd, slab, meta, meta_x, meta_y, meta_in, meta_f, tri,
    gain_p, ysend, yrecv, yprt, hid, hid_p, xsend, xrecv, psend, precv,
    w_sem, g_sem, slab_r, zs, xs, mi_r, mi_s, m_r, m_s,
    y_s, y_r, d_s, d_r, h_s, h_r, x_s, x_r, p_s, p_r,
):
    ep = lax.axis_index("ep")
    c = lax.axis_index("tp")
    x = rem(ep, X)
    y = rem(ep // X, Y)
    z = ep // (X * Y)
    group = z * Y + y

    def device(xx, yy, zz):
        return (zz * (X * Y) + yy * X + xx, c)

    def remote(src, dst, send, recv, to):
        return pltpu.make_async_remote_copy(
            src_ref=src, dst_ref=dst, send_sem=send, recv_sem=recv,
            device_id=to, device_id_type=pl.DeviceIdType.MESH,
        )

    partner = (ep, 1 - c)
    barrier = pltpu.get_barrier_semaphore()

    def greet(to):
        pl.semaphore_signal(barrier, inc=1, device_id=to, device_id_type=pl.DeviceIdType.MESH)

    greet(partner)
    for d in range(1, X):
        greet(device(rem(x + d, X), y, z))

    def greet_plane(i, carry):
        greet(device(x, rem(y + rem(i, Y), Y), rem(z + i // Y, Z)))
        return carry

    lax.fori_loop(1, Y * Z, greet_plane, 0)

    loads = []
    for k in range(2):
        h = c if k == 0 else 1 - c
        for i, (hbm, vmem, n) in enumerate(((wg_hbm, wg, HALF), (wu_hbm, wu, HALF), (wd_hbm, wd, HID))):
            loads.append(
                pltpu.make_async_copy(
                    hbm.at[:, pl.ds(pl.multiple_of(h * n, n), n)],
                    vmem.at[:, pl.ds(k * n, n)],
                    w_sem.at[k * 3 + i],
                )
            )
    for load in loads:
        load.start()

    lanes = iota((TOK, ROWS), 1) - iota((TOK, ROWS), 0)
    at_x = jnp.where(lanes == x * TOK, 1.0, 0.0).astype(BF16)
    at_y = jnp.where(lanes == y * TOK, 1.0, 0.0).astype(BF16)
    names = picks[...].astype(F32).astype(BF16)
    weight = pick_w[...]
    hi = weight.astype(BF16)
    rest = weight - hi.astype(F32)
    mid = rest.astype(BF16)
    low = (rest - mid.astype(F32)).astype(BF16)
    meta_f[...] = jnp.zeros((16, ROWS), F32)
    meta_f[8:10, :] = dot(names, at_x)
    meta_x[...] = meta_f[...].astype(BF16)
    meta_f[8:10, :] = jnp.zeros((2, ROWS), F32)
    for k, part in enumerate((names, hi, mid, low)):
        meta_f[2 * k : 2 * k + 2, :] = dot(part, at_y)
    meta_y[...] = meta_f[...].astype(BF16)
    a, b = iota((ROWS, ROWS), 0), iota((ROWS, ROWS), 1)
    tri[...] = jnp.where((a // TOK == b // TOK) & (a < b), 1.0, 0.0).astype(BF16)
    slab[0, pl.ds(pl.multiple_of(x * TOK, TOK), TOK), :] = tok[...]

    def block(b, s):
        return slab.at[b, pl.ds(pl.multiple_of(s * TOK, TOK), TOK)]

    def own_to_x(d):
        return remote(tok, block(0, x), xs.at[d], slab_r.at[0, x], device(rem(x + d, X), y, z))

    def from_x(d):
        s = rem(x + d, X)
        return remote(tok, block(0, s), xs.at[d], slab_r.at[0, s], device(s, y, z))

    def along(b, to, s, sign):
        return remote(
            block(b, s), block(to, s), zs.at[to, s], slab_r.at[to, s], device(x, y, rem(z + sign + Z, Z))
        )

    def own_along(to, sign):
        return remote(tok, block(to, x), zs.at[to, x], slab_r.at[to, x], device(x, y, rem(z + sign + Z, Z)))

    def meta_along(b, to, sign):
        return remote(meta.at[b], meta.at[to], m_s.at[to], m_r.at[to], device(x, y, rem(z + sign + Z, Z)))

    def meta_to_x(d):
        return remote(meta_x, meta_in.at[x], mi_s.at[d], mi_r.at[x], device(rem(x + d, X), y, z))

    def meta_to_y(d):
        return remote(
            meta_y, meta_in.at[X + y], mi_s.at[X + d], mi_r.at[X + y], device(x, rem(y + d, Y), z)
        )

    def meta_from(i):
        return remote(meta_x, meta_in.at[i], mi_s.at[0], mi_r.at[i], partner)

    gain_copy = remote(gain, gain_p, g_sem.at[0], g_sem.at[1], partner)

    pl.semaphore_wait(barrier, X - 1 + Y * Z - 1 + 1)

    for d in (1, 3, 2):
        meta_to_x(d).start()
        meta_to_y(d).start()
    for d in (1, 3, 2):
        own_to_x(d).start()
    own_along(1, 1).start()
    own_along(2, -1).start()
    gain_copy.start()

    for d in (1, 3, 2):
        meta_from(rem(x + d, X)).wait_recv()
        meta_from(X + rem(y + d, Y)).wait_recv()
    table = meta_x[...].astype(F32) + meta_y[...].astype(F32)
    for d in range(1, 4):
        table = table + meta_in[rem(x + d, X)].astype(F32) + meta_in[X + rem(y + d, Y)].astype(F32)
    meta[0] = table.astype(BF16)
    meta_along(0, 1, 1).start()
    meta_along(0, 2, -1).start()
    for d in (1, 3, 2):
        from_x(d).wait_recv()
        s = rem(x + d, X)
        along(0, 1, s, 1).start()
        along(0, 2, s, -1).start()

    gain_copy.wait()
    for load in loads:
        load.wait()

    def relay_cond(b, s):
        return (b <= 4) | ((b == 5) & (s < 2)) | ((b == 6) & (s >= 2))

    def relay(b):
        sign = 2 * rem(b, 2) - 1
        to = jnp.minimum(b + 2, LAST)
        meta_along(b, b, sign).wait_recv()

        @pl.when(b <= 5)
        def _():
            meta_along(b, to, sign).start()

        for s in range(X):
            along(b, b, s, sign).wait_recv()

            @pl.when(relay_cond(b, s))
            def _():
                along(b, to, s, sign).start()

    def y_message(b, d):
        t = rem(y + d, Y)
        return remote(
            ysend.at[b, pl.ds(pl.multiple_of(t * 64, 64), 64)],
            yrecv.at[b, pl.ds(pl.multiple_of(y * 64, 64), 64)],
            y_s.at[b, d], y_r.at[b, y], device(x, t, z),
        )

    def y_arrival(b, d):
        t = rem(y + d, Y)
        return remote(
            ysend.at[b, pl.ds(0, 64)],
            yrecv.at[b, pl.ds(pl.multiple_of(t * 64, 64), 64)],
            y_s.at[b, d], y_r.at[b, t], device(x, t, z),
        )

    row = iota((8, ROWS), 0)
    segment = (iota((8, ROWS), 1) // TOK).astype(F32)
    slot = iota((PACK, ROWS), 0).astype(F32)

    def select(b):
        table = meta[b].astype(F32)
        expert = (z * 32 + row // 2 * 8 + x * 2 + rem(row, 2)).astype(F32)
        hit = jnp.where((table[8:9, :] == expert) | (table[9:10, :] == expert), 1.0, 0.0)
        rank = dot(hit.astype(BF16), tri[...])
        code = jnp.where(hit > 0.0, segment * SLOTS + rank, -1.0)
        chosen = jnp.concatenate(
            [jnp.where(code[q : q + 1, :] == slot, 1.0, 0.0) for q in range(8)], axis=0
        ).astype(BF16)
        ysend[b] = dot(chosen, slab[b]).astype(BF16)
        for d in (2, 1, 3):
            y_message(b, d).start()
        mine = pl.ds(pl.multiple_of(y * 64, 64), 64)
        yrecv[b, mine, :] = ysend[b, mine, :]

    def halves(b):
        return remote(yrecv.at[b], yprt.at[b], d_s.at[b], d_r.at[b], partner)

    def swap(b):
        for d in (1, 3, 2):
            y_arrival(b, d).wait_recv()
        halves(b).start()

    def hidden_halves(b):
        return remote(hid.at[b], hid_p.at[b], h_s.at[b], h_r.at[b], partner)

    def expert_in(b):
        halves(b).wait_recv()
        own = yrecv[b].astype(F32)
        other = yprt[b].astype(F32)
        total = jnp.sum(own * own, axis=1, keepdims=True) + jnp.sum(other * other, axis=1, keepdims=True)
        scale = lax.rsqrt(total / FULL + EPS)
        rows = jnp.concatenate(
            [(own * scale * gain[...]).astype(BF16), (other * scale * gain_p[...]).astype(BF16)], axis=1
        )
        for j in range(2):
            part = jnp.concatenate(
                [rows[s * 64 + j * 32 : s * 64 + j * 32 + 32, :] for s in range(Y)], axis=0
            )
            gate = dot(part, wg[j])
            up = dot(part, wu[j])
            hid[b, j] = (gate / (1.0 + jnp.exp(-gate)) * up).astype(BF16)
        hidden_halves(b).start()

    def x_message(b, d):
        t = rem(x + d, X)
        return remote(
            xsend.at[b, pl.ds(pl.multiple_of(t * 64, 64), 64)],
            xrecv.at[b, pl.ds(pl.multiple_of(x * 64, 64), 64)],
            x_s.at[b, d], x_r.at[b, x], device(t, y, z),
        )

    def x_arrival(b, d):
        t = rem(x + d, X)
        return remote(
            xsend.at[b, pl.ds(0, 64)],
            xrecv.at[b, pl.ds(pl.multiple_of(t * 64, 64), 64)],
            x_s.at[b, d], x_r.at[b, t], device(t, y, z),
        )

    def expert_out(b):
        hidden_halves(b).wait_recv()
        for j in range(2):
            result = dot(jnp.concatenate([hid[b, j], hid_p[b, j]], axis=1), wd[j])
            for t in range(X):
                piece = jnp.concatenate(
                    [result[(s * X + t) * 8 : (s * X + t) * 8 + 8, :] for s in range(Y)], axis=0
                )
                xsend[b, t * 64 + j * 32 : t * 64 + j * 32 + 32, :] = piece.astype(BF16)
        for d in (2, 1, 3):
            x_message(b, d).start()
        mine = pl.ds(pl.multiple_of(x * 64, 64), 64)
        xrecv[b, mine, :] = xsend[b, mine, :]

    def offset(b):
        return (1 - 2 * rem(b, 2)) * ((b + 1) // 2)

    def home(b, s):
        return remote(
            psend.at[b, pl.ds(pl.multiple_of(s * PACK, PACK), PACK)],
            precv.at[pl.ds(pl.multiple_of(group * PACK, PACK), PACK)],
            p_s.at[b, s], p_r.at[group], device(x, s, rem(z + offset(b) + Z, Z)),
        )

    def combine(b):
        for d in (1, 3, 2):
            x_arrival(b, d).wait_recv()
        table = meta[b].astype(F32)
        expert = (group * 8 + row).astype(F32)
        first, second = table[0:1, :] == expert, table[1:2, :] == expert
        hit = jnp.where(first | second, 1.0, 0.0)
        here = jnp.where(
            (table[0:1, :] >= (group * 8).astype(F32)) & (table[0:1, :] < (group * 8 + 8).astype(F32)), 1.0, 0.0
        )
        ranks = dot(jnp.concatenate([hit, jnp.broadcast_to(here, (8, ROWS))], axis=0).astype(BF16), tri[...])
        code = jnp.where(hit > 0.0, segment * SLOTS + ranks[0:8, :], -1.0)
        spot = jnp.where(here > 0.0, segment[0:1, :] * PACK + ranks[8:9, :], -1.0)
        packing = jnp.where(spot == iota((Y * PACK, ROWS), 0).astype(F32), 1.0, 0.0).astype(BF16)
        rows = xrecv[b]
        total = None
        for k in range(1, 4):
            value = jnp.where(first, table[2 * k : 2 * k + 1, :], 0.0) + jnp.where(
                second, table[2 * k + 1 : 2 * k + 2, :], 0.0
            )
            spread = jnp.concatenate(
                [jnp.where(code[q : q + 1, :] == slot, value[q : q + 1, :], 0.0) for q in range(8)], axis=0
            ).astype(BF16)
            mixing = lax.dot_general(packing, spread, NT, preferred_element_type=F32).astype(BF16)
            term = dot(mixing, rows)
            total = term if total is None else total + term
        psend[b] = total.astype(BF16)
        for s in range(Y):
            @pl.when((b > 0) | (s != y))
            def _():
                home(b, s).start()

        @pl.when(b == 0)
        def _():
            precv[pl.ds(pl.multiple_of(group * PACK, PACK), PACK), :] = psend[
                0, pl.ds(pl.multiple_of(y * PACK, PACK), PACK), :
            ]

    def step(n, carry):
        @pl.when((n >= 1) & (n < BATCHES))
        def _():
            relay(n)

        @pl.when(n < BATCHES)
        def _():
            select(n)

        @pl.when((n >= 1) & (n < BATCHES + 1))
        def _():
            swap(n - 1)

        @pl.when((n >= 2) & (n < BATCHES + 2))
        def _():
            expert_out(n - 2)

        @pl.when((n >= 1) & (n < BATCHES + 1))
        def _():
            expert_in(n - 1)

        @pl.when((n >= 3) & (n < BATCHES + 3))
        def _():
            combine(n - 3)

        return carry

    lax.fori_loop(0, BATCHES + 3, step, 0)

    ids = picks[0:1, :] // 8
    idf = jnp.broadcast_to(ids.astype(F32), (8, TOK))
    ta, tb = iota((TOK, TOK), 0), iota((TOK, TOK), 1)
    eye = jnp.where(ta == tb, 1.0, 0.0).astype(BF16)
    column = lax.dot_general(eye, idf.astype(BF16), NT, preferred_element_type=F32)[:, 0:1]
    same = (column == idf[0:1, :]) & (tb < ta)
    before = jnp.sum(jnp.where(same, 1.0, 0.0), axis=1, keepdims=True)
    place = column * PACK + before
    opening = jnp.where(place == iota((TOK, Y * Z * PACK), 1).astype(F32), 1.0, 0.0).astype(BF16)

    def from_home(i, carry):
        g = rem(z + i // Y, Z) * Y + rem(y + rem(i, Y), Y)
        remote(
            psend.at[0, pl.ds(0, PACK)],
            precv.at[pl.ds(pl.multiple_of(g * PACK, PACK), PACK)],
            p_s.at[0, 0], p_r.at[g], partner,
        ).wait_recv()
        return carry

    lax.fori_loop(1, Y * Z, from_home, 0)
    out[...] = dot(opening, precv[...]).astype(BF16)

    for d in range(1, 4):
        meta_to_x(d).wait_send()
        meta_to_y(d).wait_send()
        own_to_x(d).wait_send()
    own_along(1, 1).wait_send()
    own_along(2, -1).wait_send()
    meta_along(0, 1, 1).wait_send()
    meta_along(0, 2, -1).wait_send()
    for d in range(1, 4):
        s = rem(x + d, X)
        along(0, 1, s, 1).wait_send()
        along(0, 2, s, -1).wait_send()

    def drain(b, carry):
        sign = 2 * rem(b, 2) - 1
        to = jnp.minimum(b + 2, LAST)

        @pl.when((b >= 1) & (b <= 5))
        def _():
            meta_along(b, to, sign).wait_send()

        for s in range(X):
            @pl.when((b >= 1) & relay_cond(b, s))
            def _():
                along(b, to, s, sign).wait_send()

        for d in range(1, 4):
            y_message(b, d).wait_send()
            x_message(b, d).wait_send()
        halves(b).wait_send()
        hidden_halves(b).wait_send()
        for s in range(Y):
            @pl.when((b > 0) | (s != y))
            def _():
                home(b, s).wait_send()

        return carry

    lax.fori_loop(0, BATCHES, drain, 0)


def local(tokens, norm_gain, routing, route_weight, w_gate, w_up, w_down):
    vmem = pl.BlockSpec(memory_space=pltpu.VMEM)
    anywhere = pl.BlockSpec(memory_space=pl.ANY)
    dma = pltpu.SemaphoreType.DMA
    batch = pltpu.VMEM((BATCHES, ROWS, HALF), BF16)
    return pl.pallas_call(
        kernel,
        out_shape=jax.ShapeDtypeStruct((TOK, HALF), BF16),
        in_specs=[vmem] * 4 + [anywhere] * 3,
        out_specs=vmem,
        scratch_shapes=[
            pltpu.VMEM((2, FULL, HID), BF16),
            pltpu.VMEM((2, FULL, HID), BF16),
            pltpu.VMEM((2, 2 * HID, HALF), BF16),
            batch,
            pltpu.VMEM((BATCHES, 16, ROWS), BF16),
            pltpu.VMEM((16, ROWS), BF16),
            pltpu.VMEM((16, ROWS), BF16),
            pltpu.VMEM((8, 16, ROWS), BF16),
            pltpu.VMEM((16, ROWS), F32),
            pltpu.VMEM((ROWS, ROWS), BF16),
            pltpu.VMEM((1, HALF), F32),
            batch,
            batch,
            batch,
            pltpu.VMEM((BATCHES, 2, 128, HID), BF16),
            pltpu.VMEM((BATCHES, 2, 128, HID), BF16),
            batch,
            batch,
            pltpu.VMEM((BATCHES, Y * PACK, HALF), BF16),
            pltpu.VMEM((Y * Z * PACK, HALF), BF16),
            dma((6,)),
            dma((2,)),
            dma((BATCHES, X)),
            dma((BATCHES, X)),
            dma((X,)),
            dma((8,)),
            dma((8,)),
            dma((BATCHES,)),
            dma((BATCHES,)),
            dma((BATCHES, Y)),
            dma((BATCHES, Y)),
            dma((BATCHES,)),
            dma((BATCHES,)),
            dma((BATCHES,)),
            dma((BATCHES,)),
            dma((BATCHES, X)),
            dma((BATCHES, X)),
            dma((BATCHES, Y)),
            dma((Y * Z,)),
        ],
        compiler_params=pltpu.CompilerParams(
            collective_id=0, has_side_effects=True, vmem_limit_bytes=60 << 20
        ),
    )(
        tokens, norm_gain.reshape(1, HALF), routing.T.astype(jnp.int32), route_weight.T,
        w_gate, w_up, w_down,
    )


def solution(mesh):
    in_specs = (
        P("ep", "tp"),
        P("tp"),
        P("ep", None),
        P("ep", None),
        P("ep", None, "tp"),
        P("ep", None, "tp"),
        P("ep", None, "tp"),
    )
    return jax.shard_map(
        local, mesh=mesh, in_specs=in_specs, out_specs=P("ep", "tp"), check_vma=False
    )
```

```python
import jax
import jax.numpy as jnp
from jax import lax
from jax.experimental import pallas as pl
from jax.experimental.pallas import tpu as pltpu
from jax.sharding import PartitionSpec as P

F32 = jnp.float32
BF16 = jnp.bfloat16
EPS = 1e-06

X, Y, Z = 4, 4, 8
TOK = 64
HALF = 512
FULL = 1024
HID = 256
SLOTS = 8
BATCHES = 8
ROWS = 256
OTHERS = 224
PACK = 32
LAST = BATCHES - 1

NT = (((1,), (1,)), ((), ()))
TN = (((0,), (0,)), ((), ()))

LAG_S, LAG_E, LAG_C, LAG_M = 2, 4, 6, 8


def dot(a, b):
    return jnp.dot(a, b, preferred_element_type=F32)


def iota(shape, dim):
    return lax.broadcasted_iota(jnp.int32, shape, dim)


def rem(a, n):
    return lax.rem(a, jnp.int32(n))


def kernel(
    tok, gain, picks, pick_w, wg_hbm, wu_hbm, wd_hbm, out,
    wg, wu, wd, slab, meta, meta_x, meta_y, meta_in, meta_f, tri,
    gains, ysend, yrecv, xsend, xrecv, msend, mrecv, fsend, frecv,
    w_sem, w_s, w_r, g_sem, slab_r, zs, xs, mi_r, mi_s, m_r, m_s,
    y_s, y_r, x_s, x_r, p_s, p_r, f_s, f_r,
):
    ep = lax.axis_index("ep")
    c = lax.axis_index("tp")
    x = rem(ep, X)
    y = rem(ep // X, Y)
    z = ep // (X * Y)
    group = z * Y + y

    def device(xx, yy, zz, cc=c):
        return (zz * (X * Y) + yy * X + xx, cc)

    def remote(src, dst, send, recv, to):
        return pltpu.make_async_remote_copy(
            src_ref=src, dst_ref=dst, send_sem=send, recv_sem=recv,
            device_id=to, device_id_type=pl.DeviceIdType.MESH,
        )

    def along_x(d):
        return rem(x + d, X)

    def along_y(d):
        return rem(y + d, Y)

    def along_z(d):
        return rem(z + d + Z, Z)

    def core(k):
        return rem(c + k, 2)

    partner = (ep, 1 - c)
    barrier = pltpu.get_barrier_semaphore()

    def greet(to):
        pl.semaphore_signal(barrier, inc=1, device_id=to, device_id_type=pl.DeviceIdType.MESH)

    for d in (4, 3, 5, 2, 6, 1, 7):
        greet(device(x, y, along_z(d)))
    for d in (2, 1, 3):
        for k in range(2):
            greet(device(along_x(d), y, z, core(k)))
            greet(device(x, along_y(d), z, core(k)))
    greet(partner)

    loads = [
        pltpu.make_async_copy(hbm.at[c], vmem.at[:, pl.ds(pl.multiple_of(c * n, n), n)], w_sem.at[i])
        for i, (hbm, vmem, n) in enumerate(((wg_hbm, wg, HID), (wu_hbm, wu, HID), (wd_hbm, wd, HALF)))
    ]
    gives = [
        remote(hbm.at[1 - c], vmem.at[:, pl.ds(pl.multiple_of(c * n, n), n)], w_s.at[i], w_r.at[i], partner)
        for i, (hbm, vmem, n) in enumerate(((wg_hbm, wg, HID), (wu_hbm, wu, HID), (wd_hbm, wd, HALF)))
    ]
    takes = [
        remote(hbm.at[c], vmem.at[:, pl.ds(pl.multiple_of((1 - c) * n, n), n)], w_s.at[i], w_r.at[i], partner)
        for i, (hbm, vmem, n) in enumerate(((wg_hbm, wg, HID), (wu_hbm, wu, HID), (wd_hbm, wd, HALF)))
    ]
    for load in loads:
        load.start()

    lanes = iota((TOK, ROWS), 1) - iota((TOK, ROWS), 0)
    at_x = jnp.where(lanes == x * TOK, 1.0, 0.0).astype(BF16)
    at_y = jnp.where(lanes == y * TOK, 1.0, 0.0).astype(BF16)
    names = picks[...].astype(F32).astype(BF16)
    weight = pick_w[...]
    hi = weight.astype(BF16)
    rest = weight - hi.astype(F32)
    mid = rest.astype(BF16)
    low = (rest - mid.astype(F32)).astype(BF16)
    meta_f[...] = jnp.zeros((16, ROWS), F32)
    meta_f[8:10, :] = dot(names, at_x)
    meta_x[...] = meta_f[...].astype(BF16)
    meta_f[8:10, :] = jnp.zeros((2, ROWS), F32)
    for k, part in enumerate((names, hi, mid, low)):
        meta_f[2 * k : 2 * k + 2, :] = dot(part, at_y)
    meta_y[...] = meta_f[...].astype(BF16)
    a, b = iota((ROWS, ROWS), 0), iota((ROWS, ROWS), 1)
    tri[...] = jnp.where((a // TOK == b // TOK) & (a < b), 1.0, 0.0).astype(BF16)
    slab[0, pl.ds(pl.multiple_of(x * TOK, TOK), TOK), :] = tok[...]
    gains[c] = gain[...]

    def block(b, s):
        return slab.at[b, pl.ds(pl.multiple_of(s * TOK, TOK), TOK)]

    def own_to_x(d):
        return remote(tok, block(0, x), xs.at[0], slab_r.at[0, x], device(along_x(d), y, z))

    def from_x(d):
        s = along_x(d)
        return remote(tok, block(0, s), xs.at[0], slab_r.at[0, s], device(s, y, z))

    def along(b, to, s, sign):
        return remote(
            block(b, s), block(to, s), zs.at[0], slab_r.at[to, s], device(x, y, along_z(sign))
        )

    def own_along(to, sign):
        return remote(tok, block(to, x), zs.at[0], slab_r.at[to, x], device(x, y, along_z(sign)))

    def meta_along(b, to, sign):
        return remote(meta.at[b], meta.at[to], m_s.at[0], m_r.at[to], device(x, y, along_z(sign)))

    def meta_to_x(d):
        return remote(meta_x, meta_in.at[x], mi_s.at[0], mi_r.at[0], device(along_x(d), y, z))

    def meta_to_y(d):
        return remote(meta_y, meta_in.at[X + y], mi_s.at[0], mi_r.at[0], device(x, along_y(d), z))

    meta_all = remote(meta_in.at[0:6], meta_in.at[0:6], mi_s.at[0], mi_r.at[0], partner)

    gain_give = remote(gain, gains.at[c], g_sem.at[0], g_sem.at[1], partner)
    gain_take = remote(gain, gains.at[1 - c], g_sem.at[0], g_sem.at[1], partner)

    pl.semaphore_wait(barrier, (Z - 1) + 2 * (X - 1) + 2 * (Y - 1) + 1)

    for d in (1, 3, 2):
        meta_to_x(d).start()
        meta_to_y(d).start()
    for d in (1, 3, 2):
        own_to_x(d).start()
    own_along(1, 1).start()
    own_along(2, -1).start()
    gain_give.start()
    for give in gives:
        give.start()

    meta_all.wait_recv()
    table = meta_x[...].astype(F32) + meta_y[...].astype(F32)
    for d in range(1, 4):
        table = table + meta_in[along_x(d)].astype(F32) + meta_in[X + along_y(d)].astype(F32)
    meta[0] = table.astype(BF16)
    meta_along(0, 1, 1).start()
    meta_along(0, 2, -1).start()
    for d in (1, 3, 2):
        from_x(d).wait_recv()

        @pl.when(c == 0)
        def _():
            s = along_x(d)
            along(0, 1, s, 1).start()
            along(0, 2, s, -1).start()

    def half(b, i):
        return slab.at[b, pl.ds(pl.multiple_of(x * TOK + i * 32, 32), 32)]

    def block_to_x(b, d):
        return remote(block(b, x), block(b, x), xs.at[0], slab_r.at[b, x], device(along_x(d), y, z))

    def relay(b):
        sign = 2 * rem(b, 2) - 1
        to = jnp.minimum(b + 2, LAST)
        meta_along(b, b, sign).wait_recv()

        @pl.when(b <= 5)
        def _():
            meta_along(b, to, sign).start()

        @pl.when(c == 0)
        def _():
            for s in range(X):
                along(b, b, s, sign).wait_recv()

                @pl.when((b <= 4) | ((b == 5) & (s < 2)) | ((b == 6) & (s >= 2)))
                def _():
                    along(b, to, s, sign).start()

        @pl.when(c == 1)
        def _():
            along(b, b, x, sign).wait_recv()

            @pl.when(b <= 4)
            def _():
                along(b, to, x, sign).start()

            @pl.when((b == 5) | (b == 6))
            def _():
                i = b - 5
                remote(
                    half(b, i), half(LAST, i), zs.at[0], slab_r.at[LAST, x], device(x, y, along_z(sign))
                ).start()

            for d in (2, 1, 3):
                block_to_x(b, d).start()

    def gathered(b):
        @pl.when((c == 1) & (b >= 1))
        def _():
            for d in (1, 3, 2):
                s = along_x(d)
                remote(block(b, s), block(b, s), xs.at[0], slab_r.at[b, s], device(s, y, z)).wait_recv()

    def part(i):
        return pl.ds(pl.multiple_of(i * PACK, PACK), PACK)

    PEERS = [(d, k) for d in (2, 1, 3, 0) for k in (0, 1) if (d, k) != (0, 0)]

    def y_message(b, d, k):
        t, j = along_y(d), core(k)
        return remote(
            ysend.at[b, part(t * 2 + j)], yrecv.at[b, part(c * Y + y)],
            y_s.at[0], y_r.at[b], device(x, t, z, j),
        )

    def y_arrival(b):
        return remote(ysend.at[b, 0:OTHERS], yrecv.at[b, 0:OTHERS], y_s.at[0], y_r.at[b], partner)

    row = iota((8, ROWS), 0)
    segment = (iota((8, ROWS), 1) // TOK).astype(F32)
    slot = iota((PACK, ROWS), 0).astype(F32)

    def select(b):
        gathered(b)
        table = meta[b].astype(F32)
        expert = (z * 32 + row // 2 * 8 + x * 2 + rem(row, 2)).astype(F32)
        hit = jnp.where((table[8:9, :] == expert) | (table[9:10, :] == expert), 1.0, 0.0)
        rank = dot(hit.astype(BF16), tri[...])
        code = jnp.where(hit > 0.0, segment * SLOTS + rank, -1.0)
        chosen = jnp.concatenate(
            [jnp.where(code[q : q + 1, :] == slot, 1.0, 0.0) for q in range(8)], axis=0
        ).astype(BF16)
        ysend[b] = dot(chosen, slab[b]).astype(BF16)
        for d, k in PEERS:
            y_message(b, d, k).start()
        yrecv[b, part(c * Y + y), :] = ysend[b, part(y * 2 + c), :]

    def x_message(b, d, k):
        t, h = along_x(d), core(k)
        return remote(
            xsend.at[b, part(t * 2 + h)], xrecv.at[b, part(x * 2 + c)],
            x_s.at[0], x_r.at[b], device(t, y, z, h),
        )

    def x_arrival(b):
        return remote(xsend.at[b, 0:OTHERS], xrecv.at[b, 0:OTHERS], x_s.at[0], x_r.at[b], partner)

    def expert(b):
        y_arrival(b).wait_recv()

        @pl.when(b == 0)
        def _():
            gain_take.wait_recv()
            for load in loads:
                load.wait()
            for take in takes:
                take.wait_recv()

        low, high = yrecv[b, 0:128, :].astype(F32), yrecv[b, 128:256, :].astype(F32)
        total = jnp.sum(low * low, axis=1, keepdims=True) + jnp.sum(high * high, axis=1, keepdims=True)
        scale = lax.rsqrt(total / FULL + EPS)
        rows = jnp.concatenate(
            [(low * scale * gains[0]).astype(BF16), (high * scale * gains[1]).astype(BF16)], axis=1
        )
        gate = dot(rows, wg[...])
        up = dot(rows, wu[...])
        hidden = (gate / (1.0 + jnp.exp(-gate)) * up).astype(BF16)
        result = dot(hidden, wd[...])
        for t in range(X):
            piece = jnp.concatenate(
                [result[(s * X + t) * 8 : (s * X + t) * 8 + 8, :] for s in range(Y)], axis=0
            ).astype(BF16)
            for h in range(2):
                xsend[b, (t * 2 + h) * PACK : (t * 2 + h + 1) * PACK, :] = piece[:, h * HALF : (h + 1) * HALF]
        for d, k in PEERS:
            x_message(b, d, k).start()
        xrecv[b, part(x * 2 + c), :] = xsend[b, part(x * 2 + c), :]

    def merge_message(b, d):
        t = along_y(d)
        return remote(
            msend.at[b, part(t)], mrecv.at[b, part(y)], p_s.at[0], p_r.at[b], device(x, t, z)
        )

    def merge_arrival(b):
        return remote(msend.at[b, 0:96], mrecv.at[b, 0:96], p_s.at[0], p_r.at[b], partner)

    def combine(b):
        x_arrival(b).wait_recv()
        table = meta[b].astype(F32)
        expert = (group * 8 + row).astype(F32)
        first, second = table[0:1, :] == expert, table[1:2, :] == expert
        hit = jnp.where(first | second, 1.0, 0.0)
        here = jnp.where(
            (table[0:1, :] >= (group * 8).astype(F32)) & (table[0:1, :] < (group * 8 + 8).astype(F32)), 1.0, 0.0
        )
        ranks = dot(jnp.concatenate([hit, jnp.broadcast_to(here, (8, ROWS))], axis=0).astype(BF16), tri[...])
        code = jnp.where(hit > 0.0, segment * SLOTS + ranks[0:8, :], -1.0)
        spot = jnp.where(here > 0.0, segment[0:1, :] * PACK + ranks[8:9, :], -1.0)
        packing = jnp.where(spot == iota((Y * PACK, ROWS), 0).astype(F32), 1.0, 0.0).astype(BF16)
        rows = xrecv[b]
        total = None
        for k in range(1, 4):
            value = jnp.where(first, table[2 * k : 2 * k + 1, :], 0.0) + jnp.where(
                second, table[2 * k + 1 : 2 * k + 2, :], 0.0
            )
            spread = jnp.concatenate(
                [jnp.where(code[q : q + 1, :] == slot, value[q : q + 1, :], 0.0) for q in range(8)], axis=0
            ).astype(BF16)
            mixing = lax.dot_general(packing, spread, NT, preferred_element_type=F32).astype(BF16)
            term = dot(mixing, rows)
            total = term if total is None else total + term
        msend[b] = total.astype(BF16)
        for d in (2, 1, 3):
            merge_message(b, d).start()
        mrecv[b, part(y), :] = msend[b, part(y), :]

    def offset(b):
        return (1 - 2 * rem(b, 2)) * ((b + 1) // 2)

    def home(b):
        return remote(fsend.at[b], frecv.at[z], f_s.at[0], f_r.at[0], device(x, y, along_z(offset(b))))

    def merge(b):
        merge_arrival(b).wait_recv()
        mine = jnp.where(iota((ROWS, TOK), 0) - iota((ROWS, TOK), 1) == y * TOK, 1.0, 0.0).astype(BF16)
        name = dot(meta[b], mine)[0:1, :]
        low = ((z * Y + iota((8, TOK), 0)) * 8).astype(F32)
        hit = jnp.where((name >= low) & (name < low + 8.0) & (iota((8, TOK), 0) < Y), 1.0, 0.0)
        rank = dot(hit.astype(BF16), tri[0:TOK, 0:TOK])
        code = jnp.where(hit > 0.0, rank, -1.0)
        spots = iota((PACK, TOK), 0).astype(F32)
        opening = jnp.concatenate(
            [jnp.where(code[q : q + 1, :] == spots, 1.0, 0.0) for q in range(Y)], axis=0
        ).astype(BF16)
        fsend[b] = lax.dot_general(opening, mrecv[b], TN, preferred_element_type=F32).astype(BF16)

        @pl.when(b == 0)
        def _():
            frecv[z] = fsend[0]

        @pl.when(b > 0)
        def _():
            home(b).start()

    def step(n, carry):
        def stage(lag, run):
            @pl.when((n >= lag) & (n < BATCHES + lag))
            def _():
                run(n - lag)

        stage(LAG_S, select)

        @pl.when(n < BATCHES - 1)
        def _():
            relay(n + 1)

        for lag, run in ((LAG_E, expert), (LAG_C, combine), (LAG_M, merge)):
            stage(lag, run)
        return carry

    lax.fori_loop(0, BATCHES + LAG_M, step, 0)

    homes = remote(fsend.at[0 : Z - 1], frecv.at[0 : Z - 1], f_s.at[0], f_r.at[0], partner)
    homes.wait_recv()
    total = frecv[0].astype(F32)
    for i in range(1, Z):
        total = total + frecv[i].astype(F32)
    out[...] = total.astype(BF16)

    def left(send, shape_of):
        remote(shape_of, shape_of, send, f_r.at[0], partner).wait_send()

    left(mi_s.at[0], meta_in.at[0:6])
    left(m_s.at[0], meta.at[0:7])

    @pl.when(c == 0)
    def _():
        left(zs.at[0], slab.at[0:7])
        left(xs.at[0], slab.at[0, 0:192])

    @pl.when(c == 1)
    def _():
        left(zs.at[0], slab.at[0:7, 0:TOK])
        left(xs.at[0], slab.at[0:6])

    gain_give.wait_send()
    for give in gives:
        give.wait_send()
    left(y_s.at[0], ysend.at[:, 0:OTHERS])
    left(x_s.at[0], xsend.at[:, 0:OTHERS])
    left(p_s.at[0], msend.at[:, 0:96])
    homes.wait_send()


def local(tokens, norm_gain, routing, route_weight, w_gate, w_up, w_down):
    vmem = pl.BlockSpec(memory_space=pltpu.VMEM)
    anywhere = pl.BlockSpec(memory_space=pl.ANY)
    dma = pltpu.SemaphoreType.DMA
    batch = pltpu.VMEM((BATCHES, ROWS, HALF), BF16)
    return pl.pallas_call(
        kernel,
        out_shape=jax.ShapeDtypeStruct((TOK, HALF), BF16),
        in_specs=[vmem] * 4 + [anywhere] * 3,
        out_specs=vmem,
        scratch_shapes=[
            pltpu.VMEM((FULL, 2 * HID), BF16),
            pltpu.VMEM((FULL, 2 * HID), BF16),
            pltpu.VMEM((2 * HID, FULL), BF16),
            batch,
            pltpu.VMEM((BATCHES, 16, ROWS), BF16),
            pltpu.VMEM((16, ROWS), BF16),
            pltpu.VMEM((16, ROWS), BF16),
            pltpu.VMEM((8, 16, ROWS), BF16),
            pltpu.VMEM((16, ROWS), F32),
            pltpu.VMEM((ROWS, ROWS), BF16),
            pltpu.VMEM((2, 1, HALF), F32),
            batch,
            batch,
            batch,
            batch,
            pltpu.VMEM((BATCHES, Y * PACK, HALF), BF16),
            pltpu.VMEM((BATCHES, Y * PACK, HALF), BF16),
            pltpu.VMEM((BATCHES, TOK, HALF), BF16),
            pltpu.VMEM((Z, TOK, HALF), BF16),
            dma((3,)),
            dma((3,)),
            dma((3,)),
            dma((2,)),
            dma((BATCHES, X)),
            dma((1,)),
            dma((1,)),
            dma((1,)),
            dma((1,)),
            dma((BATCHES,)),
            dma((1,)),
            dma((1,)),
            dma((BATCHES,)),
            dma((1,)),
            dma((BATCHES,)),
            dma((1,)),
            dma((BATCHES,)),
            dma((1,)),
            dma((1,)),
        ],
        compiler_params=pltpu.CompilerParams(
            collective_id=0, has_side_effects=True, vmem_limit_bytes=60 << 20
        ),
    )(
        tokens, norm_gain.reshape(1, HALF), routing.T.astype(jnp.int32), route_weight.T,
        w_gate, w_up, w_down,
    )


def solution(mesh):
    in_specs = (
        P("ep", "tp"),
        P("tp"),
        P("ep", None),
        P("ep", None),
        P("ep", None, "tp"),
        P("ep", None, "tp"),
        P("ep", None, "tp"),
    )
    return jax.shard_map(
        local, mesh=mesh, in_specs=in_specs, out_specs=P("ep", "tp"), check_vma=False
    )
```

```python
import jax
import jax.numpy as jnp
from jax import lax
from jax.experimental import pallas as pl
from jax.experimental.pallas import tpu as pltpu
from jax.sharding import PartitionSpec as P

F32 = jnp.float32
BF16 = jnp.bfloat16
EPS = 1e-06

X, Y, Z = 4, 4, 8
TOK = 64
HALF = 512
FULL = 1024
HID = 256
SLOTS = 8
BATCHES = 8
ROWS = 256
OTHERS = 224
PACK = 32
LAST = BATCHES - 1

NT = (((1,), (1,)), ((), ()))
TN = (((0,), (0,)), ((), ()))

ORDER = (
    "T0 X0 S0 U1", "U2 T1 T2 R1", "R2 U3 U4 S1", "S2 T3 T4 R3", "R4 U5 U6 S3", "E0 S4 T5 T6",
    "R5 R6 U7 S5", "E1 S6 T7 R7", "S7 E2 C0 E3", "C1 E4 C2 E5", "C3 E6 C4 E7", "M0 M1 C5 M2",
    "M3 C6 M4 C7", "M5 M6 M7",
)
FIRST = 0


def dot(a, b):
    return jnp.dot(a, b, preferred_element_type=F32)


def iota(shape, dim):
    return lax.broadcasted_iota(jnp.int32, shape, dim)


def rem(a, n):
    return lax.rem(a, jnp.int32(n))


def kernel(
    tok, gain, picks, pick_w, wg_hbm, wu_hbm, wd_hbm, out,
    wg, wu, wd, slab, meta, meta_x, meta_y, meta_in, meta_f, tri,
    gains, chosen, mixing, opening, ysend, yrecv, xsend, xrecv, msend, mrecv, fsend, frecv,
    w_sem, w_s, w_r, g_sem, slab_r, zs, xs, mi_r, mi_s, m_r, m_s,
    y_s, y_r, x_s, x_r, p_s, p_r, f_s, f_r,
):
    ep = lax.axis_index("ep")
    c = lax.axis_index("tp")
    x = rem(ep, X)
    y = rem(ep // X, Y)
    z = ep // (X * Y)
    group = z * Y + y

    def device(xx, yy, zz, cc=c):
        return (zz * (X * Y) + yy * X + xx, cc)

    def remote(src, dst, send, recv, to):
        return pltpu.make_async_remote_copy(
            src_ref=src, dst_ref=dst, send_sem=send, recv_sem=recv,
            device_id=to, device_id_type=pl.DeviceIdType.MESH,
        )

    def along_x(d):
        return rem(x + d, X)

    def along_y(d):
        return rem(y + d, Y)

    def along_z(d):
        return rem(z + d + Z, Z)

    def core(k):
        return rem(c + k, 2)

    def offset(b):
        return (1 - 2 * (b % 2)) * ((b + 1) // 2)

    partner = (ep, 1 - c)
    barrier = pltpu.get_barrier_semaphore()

    def greet(to):
        pl.semaphore_signal(barrier, inc=1, device_id=to, device_id_type=pl.DeviceIdType.MESH)

    for d in (4, 3, 5, 2, 6, 1, 7):
        greet(device(x, y, along_z(d)))
    for d in (2, 1, 3):
        for k in range(2):
            greet(device(along_x(d), y, z, core(k)))
            greet(device(x, along_y(d), z, core(k)))
    greet(partner)

    loads = [
        pltpu.make_async_copy(hbm.at[c], vmem.at[:, pl.ds(pl.multiple_of(c * n, n), n)], w_sem.at[i])
        for i, (hbm, vmem, n) in enumerate(((wg_hbm, wg, HID), (wu_hbm, wu, HID), (wd_hbm, wd, HALF)))
    ]
    gives = [
        remote(hbm.at[1 - c], vmem.at[:, pl.ds(pl.multiple_of(c * n, n), n)], w_s.at[i], w_r.at[i], partner)
        for i, (hbm, vmem, n) in enumerate(((wg_hbm, wg, HID), (wu_hbm, wu, HID), (wd_hbm, wd, HALF)))
    ]
    takes = [
        remote(hbm.at[c], vmem.at[:, pl.ds(pl.multiple_of((1 - c) * n, n), n)], w_s.at[i], w_r.at[i], partner)
        for i, (hbm, vmem, n) in enumerate(((wg_hbm, wg, HID), (wu_hbm, wu, HID), (wd_hbm, wd, HALF)))
    ]
    for load in loads:
        load.start()

    lanes = iota((TOK, ROWS), 1) - iota((TOK, ROWS), 0)
    at_x = jnp.where(lanes == x * TOK, 1.0, 0.0).astype(BF16)
    at_y = jnp.where(lanes == y * TOK, 1.0, 0.0).astype(BF16)
    names = picks[...].astype(F32).astype(BF16)
    weight = pick_w[...]
    hi = weight.astype(BF16)
    rest = weight - hi.astype(F32)
    mid = rest.astype(BF16)
    low = (rest - mid.astype(F32)).astype(BF16)
    meta_f[...] = jnp.zeros((16, ROWS), F32)
    meta_f[8:10, :] = dot(names, at_x)
    meta_x[...] = meta_f[...].astype(BF16)
    meta_f[8:10, :] = jnp.zeros((2, ROWS), F32)
    for k, part in enumerate((names, hi, mid, low)):
        meta_f[2 * k : 2 * k + 2, :] = dot(part, at_y)
    meta_y[...] = meta_f[...].astype(BF16)
    a, b = iota((ROWS, ROWS), 0), iota((ROWS, ROWS), 1)
    tri[...] = jnp.where((a // TOK == b // TOK) & (a < b), 1.0, 0.0).astype(BF16)
    slab[0, pl.ds(pl.multiple_of(x * TOK, TOK), TOK), :] = tok[...]
    gains[c] = gain[...]

    def block(b, s):
        return slab.at[b, pl.ds(pl.multiple_of(s * TOK, TOK), TOK)]

    def own_to_x(d):
        return remote(tok, block(0, x), xs.at[0], slab_r.at[0, x], device(along_x(d), y, z))

    def from_x(d):
        s = along_x(d)
        return remote(tok, block(0, s), xs.at[0], slab_r.at[0, s], device(s, y, z))

    def along(b, to, s, sign):
        return remote(
            block(b, s), block(to, s), zs.at[0], slab_r.at[to, s], device(x, y, along_z(sign))
        )

    def own_along(to, sign):
        return remote(tok, block(to, x), zs.at[0], slab_r.at[to, x], device(x, y, along_z(sign)))

    def meta_along(b, to, sign):
        return remote(meta.at[b], meta.at[to], m_s.at[0], m_r.at[to], device(x, y, along_z(sign)))

    def meta_to_x(d):
        return remote(meta_x, meta_in.at[x], mi_s.at[0], mi_r.at[0], device(along_x(d), y, z))

    def meta_to_y(d):
        return remote(meta_y, meta_in.at[X + y], mi_s.at[0], mi_r.at[0], device(x, along_y(d), z))

    meta_all = remote(meta_in.at[0:6], meta_in.at[0:6], mi_s.at[0], mi_r.at[0], partner)

    gain_give = remote(gain, gains.at[c], g_sem.at[0], g_sem.at[1], partner)
    gain_take = remote(gain, gains.at[1 - c], g_sem.at[0], g_sem.at[1], partner)

    pl.semaphore_wait(barrier, (Z - 1) + 2 * (X - 1) + 2 * (Y - 1) + 1)

    for d in (1, 3, 2):
        meta_to_x(d).start()
        meta_to_y(d).start()
    for d in (1, 3, 2):
        own_to_x(d).start()
    @pl.when(c == 0)
    def _():
        own_along(1, 1).start()
        own_along(2, -1).start()

    @pl.when(c == 1)
    def _():
        for b in range(1, BATCHES):
            own_along(b, -offset(b)).start()

    gain_give.start()
    for give in gives:
        give.start()

    meta_all.wait_recv()
    table = meta_x[...].astype(F32) + meta_y[...].astype(F32)
    for d in range(1, 4):
        table = table + meta_in[along_x(d)].astype(F32) + meta_in[X + along_y(d)].astype(F32)
    meta[0] = table.astype(BF16)
    meta_along(0, 1, 1).start()
    meta_along(0, 2, -1).start()

    def own_blocks():
        for d in (1, 3, 2):
            own_block(d)

    def own_block(d):
        from_x(d).wait_recv()

        @pl.when(c == 0)
        def _():
            s = along_x(d)
            along(0, 1, s, 1).start()
            along(0, 2, s, -1).start()

    def block_to_x(b, d):
        return remote(block(b, x), block(b, x), xs.at[0], slab_r.at[b, x], device(along_x(d), y, z))

    def tables(b):
        if b > 0:
            sign = 1 if b % 2 else -1
            meta_along(b, b, sign).wait_recv()
            if b <= 5:
                meta_along(b, b + 2, sign).start()
        prepare(b)

    def relay(b):
        sign = 1 if b % 2 else -1
        to = min(b + 2, LAST)

        @pl.when(c == 0)
        def _():
            for s in range(X):
                along(b, b, s, sign).wait_recv()
                if b <= 4 or (b == 5 and s < 2) or (b == 6 and s >= 2):
                    along(b, to, s, sign).start()

    def spread(b):
        @pl.when(c == 1)
        def _():
            along(b, b, x, 1).wait_recv()
            for d in (2, 1, 3):
                block_to_x(b, d).start()

    def gathered(b):
        if b == 0:
            return

        @pl.when(c == 1)
        def _():
            for d in (1, 3, 2):
                s = along_x(d)
                remote(block(b, s), block(b, s), xs.at[0], slab_r.at[b, s], device(s, y, z)).wait_recv()

    def part(i):
        return pl.ds(pl.multiple_of(i * PACK, PACK), PACK)

    PEERS = [(d, k) for d in (2, 1, 3, 0) for k in (0, 1) if (d, k) != (0, 0)]

    def y_message(b, d, k):
        t, j = along_y(d), core(k)
        return remote(
            ysend.at[b, part(t * 2 + j)], yrecv.at[b, part(c * Y + y)],
            y_s.at[0], y_r.at[b], device(x, t, z, j),
        )

    def y_arrival(b):
        return remote(ysend.at[b, 0:OTHERS], yrecv.at[b, 0:OTHERS], y_s.at[0], y_r.at[b], partner)

    row = iota((8, ROWS), 0)
    segment = (iota((8, ROWS), 1) // TOK).astype(F32)
    slot = iota((PACK, ROWS), 0).astype(F32)

    def spread_out(code, value):
        return jnp.concatenate(
            [jnp.where(code[q : q + 1, :] == slot, value[q : q + 1, :], 0.0) for q in range(8)], axis=0
        ).astype(BF16)

    def prepare(b):
        table = meta[b].astype(F32)
        expert = (z * 32 + row // 2 * 8 + x * 2 + rem(row, 2)).astype(F32)
        hit = jnp.where((table[8:9, :] == expert) | (table[9:10, :] == expert), 1.0, 0.0)
        member = (group * 8 + row).astype(F32)
        first, second = table[0:1, :] == member, table[1:2, :] == member
        hit_here = jnp.where(first | second, 1.0, 0.0)
        low = ((z * Y + row) * 8).astype(F32)
        hit_z = jnp.where((table[0:1, :] >= low) & (table[0:1, :] < low + 8.0) & (row < Y), 1.0, 0.0)
        ranks = dot(jnp.concatenate([hit, hit_here, hit_z, hit_z], axis=0).astype(BF16), tri[...])
        chosen[b] = spread_out(
            jnp.where(hit > 0.0, segment * SLOTS + ranks[0:8, :], -1.0), jnp.ones((8, ROWS), F32)
        )
        code = jnp.where(hit_here > 0.0, segment * SLOTS + ranks[8:16, :], -1.0)
        rank_z = jnp.where(hit_z > 0.0, ranks[16:24, :], -1.0)
        spot = jnp.sum(
            jnp.where((row == y) & (hit_z > 0.0), segment * PACK + ranks[16:24, :] + 1.0, 0.0), axis=0, keepdims=True
        )
        packing = jnp.where(spot - 1.0 == iota((Y * PACK, ROWS), 0).astype(F32), 1.0, 0.0).astype(BF16)
        for k in range(1, 4):
            value = jnp.where(first, table[2 * k : 2 * k + 1, :], 0.0) + jnp.where(
                second, table[2 * k + 1 : 2 * k + 2, :], 0.0
            )
            mixing[b, k - 1] = lax.dot_general(
                packing, spread_out(code, value), NT, preferred_element_type=F32
            ).astype(BF16)
        mine = jnp.where(iota((ROWS, TOK), 0) - iota((ROWS, TOK), 1) == y * TOK, 1.0, 0.0).astype(BF16)
        own = dot(rank_z.astype(BF16), mine)
        spots = iota((PACK, TOK), 0).astype(F32)
        opening[b] = jnp.concatenate(
            [jnp.where(own[q : q + 1, :] == spots, 1.0, 0.0) for q in range(Y)], axis=0
        ).astype(BF16)

    def select(b):
        gathered(b)
        ysend[b] = dot(chosen[b], slab[b]).astype(BF16)
        for d, k in PEERS:
            y_message(b, d, k).start()
        yrecv[b, part(c * Y + y), :] = ysend[b, part(y * 2 + c), :]

    def x_message(b, d, k):
        t, h = along_x(d), core(k)
        return remote(
            xsend.at[b, part(t * 2 + h)], xrecv.at[b, part(x * 2 + c)],
            x_s.at[0], x_r.at[b], device(t, y, z, h),
        )

    def x_arrival(b):
        return remote(xsend.at[b, 0:OTHERS], xrecv.at[b, 0:OTHERS], x_s.at[0], x_r.at[b], partner)

    def expert(b):
        y_arrival(b).wait_recv()

        if b == FIRST:
            gain_take.wait_recv()
            for load in loads:
                load.wait()
            for take in takes:
                take.wait_recv()

        low, high = yrecv[b, 0:128, :].astype(F32), yrecv[b, 128:256, :].astype(F32)
        total = jnp.sum(low * low, axis=1, keepdims=True) + jnp.sum(high * high, axis=1, keepdims=True)
        scale = lax.rsqrt(total / FULL + EPS)
        rows = jnp.concatenate(
            [(low * scale * gains[0]).astype(BF16), (high * scale * gains[1]).astype(BF16)], axis=1
        )
        gate = dot(rows, wg[...])
        up = dot(rows, wu[...])
        hidden = (gate / (1.0 + jnp.exp(-gate)) * up).astype(BF16)
        result = dot(hidden, wd[...])
        for t in range(X):
            piece = jnp.concatenate(
                [result[(s * X + t) * 8 : (s * X + t) * 8 + 8, :] for s in range(Y)], axis=0
            ).astype(BF16)
            for h in range(2):
                xsend[b, (t * 2 + h) * PACK : (t * 2 + h + 1) * PACK, :] = piece[:, h * HALF : (h + 1) * HALF]
        for d, k in PEERS:
            x_message(b, d, k).start()
        xrecv[b, part(x * 2 + c), :] = xsend[b, part(x * 2 + c), :]

    def merge_message(b, d):
        t = along_y(d)
        return remote(
            msend.at[b, part(t)], mrecv.at[b, part(y)], p_s.at[0], p_r.at[b], device(x, t, z)
        )

    def merge_arrival(b):
        return remote(msend.at[b, 0:96], mrecv.at[b, 0:96], p_s.at[0], p_r.at[b], partner)

    def combine(b):
        x_arrival(b).wait_recv()
        rows = xrecv[b]
        total = dot(mixing[b, 0], rows) + dot(mixing[b, 1], rows) + dot(mixing[b, 2], rows)
        msend[b] = total.astype(BF16)
        for d in (2, 1, 3):
            merge_message(b, d).start()
        mrecv[b, part(y), :] = msend[b, part(y), :]

    def home(b):
        return remote(fsend.at[b], frecv.at[z], f_s.at[0], f_r.at[0], device(x, y, along_z(offset(b))))

    def merge(b):
        merge_arrival(b).wait_recv()
        fsend[b] = lax.dot_general(opening[b], mrecv[b], TN, preferred_element_type=F32).astype(BF16)
        if b == 0:
            frecv[z] = fsend[0]
        else:
            home(b).start()

    stages = dict(X=lambda b: own_blocks(), T=tables, U=spread, R=relay, S=select, E=expert, C=combine, M=merge)
    for name in " ".join(ORDER).split():
        run, n = stages[name[0]], int(name[1])
        run(n)

    homes = remote(fsend.at[0 : Z - 1], frecv.at[0 : Z - 1], f_s.at[0], f_r.at[0], partner)
    homes.wait_recv()
    total = frecv[0].astype(F32)
    for i in range(1, Z):
        total = total + frecv[i].astype(F32)
    out[...] = total.astype(BF16)

    def left(send, shape_of):
        remote(shape_of, shape_of, send, f_r.at[0], partner).wait_send()

    left(mi_s.at[0], meta_in.at[0:6])
    left(m_s.at[0], meta.at[0:7])

    @pl.when(c == 0)
    def _():
        left(zs.at[0], slab.at[0:7])
        left(xs.at[0], slab.at[0, 0:192])

    @pl.when(c == 1)
    def _():
        left(zs.at[0], slab.at[0:7, 0:TOK])
        left(xs.at[0], slab.at[0:6])

    gain_give.wait_send()
    for give in gives:
        give.wait_send()
    left(y_s.at[0], ysend.at[:, 0:OTHERS])
    left(x_s.at[0], xsend.at[:, 0:OTHERS])
    left(p_s.at[0], msend.at[:, 0:96])
    homes.wait_send()


def local(tokens, norm_gain, routing, route_weight, w_gate, w_up, w_down):
    vmem = pl.BlockSpec(memory_space=pltpu.VMEM)
    anywhere = pl.BlockSpec(memory_space=pl.ANY)
    dma = pltpu.SemaphoreType.DMA
    batch = pltpu.VMEM((BATCHES, ROWS, HALF), BF16)
    return pl.pallas_call(
        kernel,
        out_shape=jax.ShapeDtypeStruct((TOK, HALF), BF16),
        in_specs=[vmem] * 4 + [anywhere] * 3,
        out_specs=vmem,
        scratch_shapes=[
            pltpu.VMEM((FULL, 2 * HID), BF16),
            pltpu.VMEM((FULL, 2 * HID), BF16),
            pltpu.VMEM((2 * HID, FULL), BF16),
            batch,
            pltpu.VMEM((BATCHES, 16, ROWS), BF16),
            pltpu.VMEM((16, ROWS), BF16),
            pltpu.VMEM((16, ROWS), BF16),
            pltpu.VMEM((8, 16, ROWS), BF16),
            pltpu.VMEM((16, ROWS), F32),
            pltpu.VMEM((ROWS, ROWS), BF16),
            pltpu.VMEM((2, 1, HALF), F32),
            pltpu.VMEM((BATCHES, ROWS, ROWS), BF16),
            pltpu.VMEM((BATCHES, 3, Y * PACK, ROWS), BF16),
            pltpu.VMEM((BATCHES, Y * PACK, TOK), BF16),
            batch,
            batch,
            batch,
            batch,
            pltpu.VMEM((BATCHES, Y * PACK, HALF), BF16),
            pltpu.VMEM((BATCHES, Y * PACK, HALF), BF16),
            pltpu.VMEM((BATCHES, TOK, HALF), BF16),
            pltpu.VMEM((Z, TOK, HALF), BF16),
            dma((3,)),
            dma((3,)),
            dma((3,)),
            dma((2,)),
            dma((BATCHES, X)),
            dma((1,)),
            dma((1,)),
            dma((1,)),
            dma((1,)),
            dma((BATCHES,)),
            dma((1,)),
            dma((1,)),
            dma((BATCHES,)),
            dma((1,)),
            dma((BATCHES,)),
            dma((1,)),
            dma((BATCHES,)),
            dma((1,)),
            dma((1,)),
        ],
        compiler_params=pltpu.CompilerParams(
            collective_id=0, has_side_effects=True, vmem_limit_bytes=60 << 20
        ),
    )(
        tokens, norm_gain.reshape(1, HALF), routing.T.astype(jnp.int32), route_weight.T,
        w_gate, w_up, w_down,
    )


def solution(mesh):
    in_specs = (
        P("ep", "tp"),
        P("tp"),
        P("ep", None),
        P("ep", None),
        P("ep", None, "tp"),
        P("ep", None, "tp"),
        P("ep", None, "tp"),
    )
    return jax.shard_map(
        local, mesh=mesh, in_specs=in_specs, out_specs=P("ep", "tp"), check_vma=False
    )
```

```python
import jax
import jax.numpy as jnp
from jax import lax
from jax.experimental import pallas as pl
from jax.experimental.pallas import tpu as pltpu
from jax.sharding import PartitionSpec as P

F32 = jnp.float32
BF16 = jnp.bfloat16
EPS = 1e-06

X, Y, Z = 4, 4, 8
TOK = 64
HALF = 512
FULL = 1024
HID = 256
SLOTS = 8
BATCHES = 8
ROWS = 256
OTHERS = 224
PACK = 32
LAST = BATCHES - 1

NT = (((1,), (1,)), ((), ()))
TN = (((0,), (0,)), ((), ()))

ORDER = (
    "T0 X0 S0 U1", "U2 T1 T2 R1", "R2 U3 U4 S1", "S2 E0 T3 T4", "U5 U6 U7 R3", "R4 S3 S4 E1",
    "T5 T6 E2 R5", "R6 S5 S6 T7", "E3 R7 S7 C0", "E4 C1 E5 C2", "E6 C3 M0 C4", "E7 M1 M2 C5",
    "M3 C6 M4 M5", "C7 M6 M7",
)
FIRST = 0


def dot(a, b):
    return jnp.dot(a, b, preferred_element_type=F32)


def iota(shape, dim):
    return lax.broadcasted_iota(jnp.int32, shape, dim)


def rem(a, n):
    return lax.rem(a, jnp.int32(n))


def kernel(
    tok_hbm, gain_hbm, picks_hbm, pick_w_hbm, wg_hbm, wu_hbm, wd_hbm, out,
    tok, gain, picks, pick_w, wg, wu, wd, slab, meta, meta_x, meta_y, meta_in, meta_f, tri,
    gains, chosen, mixing, opening, ysend, yrecv, xsend, xrecv, msend, mrecv, fsend, frecv,
    in_sem, w_sem, w_s, w_r, g_sem, slab_r, zs, xs, mi_r, mi_s, m_r, m_s,
    y_s, y_r, x_s, x_r, p_s, p_r, f_s, f_r,
):
    ep = lax.axis_index("ep")
    c = lax.axis_index("tp")
    x = rem(ep, X)
    y = rem(ep // X, Y)
    z = ep // (X * Y)
    group = z * Y + y

    def device(xx, yy, zz, cc=c):
        return (zz * (X * Y) + yy * X + xx, cc)

    def remote(src, dst, send, recv, to):
        return pltpu.make_async_remote_copy(
            src_ref=src, dst_ref=dst, send_sem=send, recv_sem=recv,
            device_id=to, device_id_type=pl.DeviceIdType.MESH,
        )

    def along_x(d):
        return rem(x + d, X)

    def along_y(d):
        return rem(y + d, Y)

    def along_z(d):
        return rem(z + d + Z, Z)

    def core(k):
        return rem(c + k, 2)

    def offset(b):
        return (1 - 2 * (b % 2)) * ((b + 1) // 2)

    partner = (ep, 1 - c)
    barrier = pltpu.get_barrier_semaphore()

    def greet(to):
        pl.semaphore_signal(barrier, inc=1, device_id=to, device_id_type=pl.DeviceIdType.MESH)

    for d in (4, 3, 5, 2, 6, 1, 7):
        greet(device(x, y, along_z(d)))
    for d in (2, 1, 3):
        for k in range(2):
            greet(device(along_x(d), y, z, core(k)))
            greet(device(x, along_y(d), z, core(k)))
    greet(partner)

    inputs = [
        pltpu.make_async_copy(hbm, vmem, in_sem.at[i])
        for i, (hbm, vmem) in enumerate(
            ((picks_hbm, picks), (pick_w_hbm, pick_w), (tok_hbm, tok), (gain_hbm, gain))
        )
    ]
    for copy in inputs:
        copy.start()

    loads = [
        pltpu.make_async_copy(hbm.at[c], vmem.at[:, pl.ds(pl.multiple_of(c * n, n), n)], w_sem.at[i])
        for i, (hbm, vmem, n) in enumerate(((wg_hbm, wg, HID), (wu_hbm, wu, HID), (wd_hbm, wd, HALF)))
    ]
    gives = [
        remote(hbm.at[1 - c], vmem.at[:, pl.ds(pl.multiple_of(c * n, n), n)], w_s.at[i], w_r.at[i], partner)
        for i, (hbm, vmem, n) in enumerate(((wg_hbm, wg, HID), (wu_hbm, wu, HID), (wd_hbm, wd, HALF)))
    ]
    takes = [
        remote(hbm.at[c], vmem.at[:, pl.ds(pl.multiple_of((1 - c) * n, n), n)], w_s.at[i], w_r.at[i], partner)
        for i, (hbm, vmem, n) in enumerate(((wg_hbm, wg, HID), (wu_hbm, wu, HID), (wd_hbm, wd, HALF)))
    ]
    for load in loads:
        load.start()

    for copy in inputs:
        copy.wait()
    lanes = iota((TOK, ROWS), 1) - iota((TOK, ROWS), 0)
    at_x = jnp.where(lanes == x * TOK, 1.0, 0.0).astype(BF16)
    at_y = jnp.where(lanes == y * TOK, 1.0, 0.0).astype(BF16)
    names = picks[...].astype(F32).astype(BF16)
    weight = pick_w[...]
    hi = weight.astype(BF16)
    rest = weight - hi.astype(F32)
    mid = rest.astype(BF16)
    low = (rest - mid.astype(F32)).astype(BF16)
    meta_f[...] = jnp.zeros((16, ROWS), F32)
    meta_f[8:10, :] = dot(names, at_x)
    meta_x[...] = meta_f[...].astype(BF16)
    meta_f[8:10, :] = jnp.zeros((2, ROWS), F32)
    for k, part in enumerate((names, hi, mid, low)):
        meta_f[2 * k : 2 * k + 2, :] = dot(part, at_y)
    meta_y[...] = meta_f[...].astype(BF16)
    a, b = iota((ROWS, ROWS), 0), iota((ROWS, ROWS), 1)
    tri[...] = jnp.where((a // TOK == b // TOK) & (a < b), 1.0, 0.0).astype(BF16)
    slab[0, pl.ds(pl.multiple_of(x * TOK, TOK), TOK), :] = tok[...]
    gains[c] = gain[...]

    def block(b, s):
        return slab.at[b, pl.ds(pl.multiple_of(s * TOK, TOK), TOK)]

    def own_to_x(d):
        return remote(tok, block(0, x), xs.at[0], slab_r.at[0, x], device(along_x(d), y, z))

    def from_x(d):
        s = along_x(d)
        return remote(tok, block(0, s), xs.at[0], slab_r.at[0, s], device(s, y, z))

    def along(b, to, s, sign):
        return remote(
            block(b, s), block(to, s), zs.at[0], slab_r.at[to, s], device(x, y, along_z(sign))
        )

    def own_along(to, sign):
        return remote(tok, block(to, x), zs.at[0], slab_r.at[to, x], device(x, y, along_z(sign)))

    def meta_along(b, to, sign):
        return remote(meta.at[b], meta.at[to], m_s.at[0], m_r.at[to], device(x, y, along_z(sign)))

    def meta_to_x(d):
        return remote(meta_x, meta_in.at[x], mi_s.at[0], mi_r.at[0], device(along_x(d), y, z))

    def meta_to_y(d):
        return remote(meta_y, meta_in.at[X + y], mi_s.at[0], mi_r.at[0], device(x, along_y(d), z))

    meta_all = remote(meta_in.at[0:6], meta_in.at[0:6], mi_s.at[0], mi_r.at[0], partner)

    gain_give = remote(gain, gains.at[c], g_sem.at[0], g_sem.at[1], partner)
    gain_take = remote(gain, gains.at[1 - c], g_sem.at[0], g_sem.at[1], partner)

    pl.semaphore_wait(barrier, (Z - 1) + 2 * (X - 1) + 2 * (Y - 1) + 1)

    for d in (1, 3, 2):
        meta_to_x(d).start()
        meta_to_y(d).start()
    for d in (1, 3, 2):
        own_to_x(d).start()
    @pl.when(c == 0)
    def _():
        own_along(1, 1).start()
        own_along(2, -1).start()

    @pl.when(c == 1)
    def _():
        for b in range(1, BATCHES):
            own_along(b, -offset(b)).start()

    gain_give.start()
    for give in gives:
        give.start()

    meta_all.wait_recv()
    table = meta_x[...].astype(F32) + meta_y[...].astype(F32)
    for d in range(1, 4):
        table = table + meta_in[along_x(d)].astype(F32) + meta_in[X + along_y(d)].astype(F32)
    meta[0] = table.astype(BF16)
    meta_along(0, 1, 1).start()
    meta_along(0, 2, -1).start()

    def own_blocks():
        for d in (1, 3, 2):
            own_block(d)

    def own_block(d):
        from_x(d).wait_recv()

        @pl.when(c == 0)
        def _():
            s = along_x(d)
            along(0, 1, s, 1).start()
            along(0, 2, s, -1).start()

    def block_to_x(b, d):
        return remote(block(b, x), block(b, x), xs.at[0], slab_r.at[b, x], device(along_x(d), y, z))

    def tables(b):
        if b > 0:
            sign = 1 if b % 2 else -1
            meta_along(b, b, sign).wait_recv()
            if b <= 5:
                meta_along(b, b + 2, sign).start()
        prepare(b)

    def relay(b):
        sign = 1 if b % 2 else -1
        to = min(b + 2, LAST)

        @pl.when(c == 0)
        def _():
            for s in range(X):
                along(b, b, s, sign).wait_recv()
                if b <= 4 or (b == 5 and s < 2) or (b == 6 and s >= 2):
                    along(b, to, s, sign).start()

    def spread(b):
        @pl.when(c == 1)
        def _():
            along(b, b, x, 1).wait_recv()
            for d in (2, 1, 3):
                block_to_x(b, d).start()

    def gathered(b):
        if b == 0:
            return

        @pl.when(c == 1)
        def _():
            for d in (1, 3, 2):
                s = along_x(d)
                remote(block(b, s), block(b, s), xs.at[0], slab_r.at[b, s], device(s, y, z)).wait_recv()

    def part(i):
        return pl.ds(pl.multiple_of(i * PACK, PACK), PACK)

    PEERS = [(d, k) for d in (2, 1, 3, 0) for k in (0, 1) if (d, k) != (0, 0)]

    def y_message(b, d, k):
        t, j = along_y(d), core(k)
        return remote(
            ysend.at[b, part(t * 2 + j)], yrecv.at[b, part(c * Y + y)],
            y_s.at[0], y_r.at[b], device(x, t, z, j),
        )

    def y_arrival(b):
        return remote(ysend.at[b, 0:OTHERS], yrecv.at[b, 0:OTHERS], y_s.at[0], y_r.at[b], partner)

    row = iota((8, ROWS), 0)
    segment = (iota((8, ROWS), 1) // TOK).astype(F32)
    slot = iota((PACK, ROWS), 0).astype(F32)

    def spread_out(code, value):
        return jnp.concatenate(
            [jnp.where(code[q : q + 1, :] == slot, value[q : q + 1, :], 0.0) for q in range(8)], axis=0
        ).astype(BF16)

    def prepare(b):
        table = meta[b].astype(F32)
        expert = (z * 32 + row // 2 * 8 + x * 2 + rem(row, 2)).astype(F32)
        hit = jnp.where((table[8:9, :] == expert) | (table[9:10, :] == expert), 1.0, 0.0)
        member = (group * 8 + row).astype(F32)
        first, second = table[0:1, :] == member, table[1:2, :] == member
        hit_here = jnp.where(first | second, 1.0, 0.0)
        low = ((z * Y + row) * 8).astype(F32)
        hit_z = jnp.where((table[0:1, :] >= low) & (table[0:1, :] < low + 8.0) & (row < Y), 1.0, 0.0)
        ranks = dot(jnp.concatenate([hit, hit_here, hit_z, hit_z], axis=0).astype(BF16), tri[...])
        chosen[b] = spread_out(
            jnp.where(hit > 0.0, segment * SLOTS + ranks[0:8, :], -1.0), jnp.ones((8, ROWS), F32)
        )
        code = jnp.where(hit_here > 0.0, segment * SLOTS + ranks[8:16, :], -1.0)
        rank_z = jnp.where(hit_z > 0.0, ranks[16:24, :], -1.0)
        spot = jnp.sum(
            jnp.where((row == y) & (hit_z > 0.0), segment * PACK + ranks[16:24, :] + 1.0, 0.0), axis=0, keepdims=True
        )
        packing = jnp.where(spot - 1.0 == iota((Y * PACK, ROWS), 0).astype(F32), 1.0, 0.0).astype(BF16)
        for k in range(1, 4):
            value = jnp.where(first, table[2 * k : 2 * k + 1, :], 0.0) + jnp.where(
                second, table[2 * k + 1 : 2 * k + 2, :], 0.0
            )
            mixing[b, k - 1] = lax.dot_general(
                packing, spread_out(code, value), NT, preferred_element_type=F32
            ).astype(BF16)
        mine = jnp.where(iota((ROWS, TOK), 0) - iota((ROWS, TOK), 1) == y * TOK, 1.0, 0.0).astype(BF16)
        own = dot(rank_z.astype(BF16), mine)
        spots = iota((PACK, TOK), 0).astype(F32)
        opening[b] = jnp.concatenate(
            [jnp.where(own[q : q + 1, :] == spots, 1.0, 0.0) for q in range(Y)], axis=0
        ).astype(BF16)

    def select(b):
        gathered(b)
        ysend[b] = dot(chosen[b], slab[b]).astype(BF16)
        for d, k in PEERS:
            y_message(b, d, k).start()
        yrecv[b, part(c * Y + y), :] = ysend[b, part(y * 2 + c), :]

    def x_message(b, d, k):
        t, h = along_x(d), core(k)
        return remote(
            xsend.at[b, part(t * 2 + h)], xrecv.at[b, part(x * 2 + c)],
            x_s.at[0], x_r.at[b], device(t, y, z, h),
        )

    def x_arrival(b):
        return remote(xsend.at[b, 0:OTHERS], xrecv.at[b, 0:OTHERS], x_s.at[0], x_r.at[b], partner)

    def expert(b):
        y_arrival(b).wait_recv()

        if b == FIRST:
            gain_take.wait_recv()
            for load in loads:
                load.wait()
            for take in takes:
                take.wait_recv()

        low, high = yrecv[b, 0:128, :].astype(F32), yrecv[b, 128:256, :].astype(F32)
        total = jnp.sum(low * low, axis=1, keepdims=True) + jnp.sum(high * high, axis=1, keepdims=True)
        scale = lax.rsqrt(total / FULL + EPS)
        rows = jnp.concatenate(
            [(low * scale * gains[0]).astype(BF16), (high * scale * gains[1]).astype(BF16)], axis=1
        )
        gate = dot(rows, wg[...])
        up = dot(rows, wu[...])
        hidden = (gate / (1.0 + jnp.exp(-gate)) * up).astype(BF16)
        result = dot(hidden, wd[...])
        for t in range(X):
            piece = jnp.concatenate(
                [result[(s * X + t) * 8 : (s * X + t) * 8 + 8, :] for s in range(Y)], axis=0
            ).astype(BF16)
            for h in range(2):
                xsend[b, (t * 2 + h) * PACK : (t * 2 + h + 1) * PACK, :] = piece[:, h * HALF : (h + 1) * HALF]
        for d, k in PEERS:
            x_message(b, d, k).start()
        xrecv[b, part(x * 2 + c), :] = xsend[b, part(x * 2 + c), :]

    def merge_message(b, d):
        t = along_y(d)
        return remote(
            msend.at[b, part(t)], mrecv.at[b, part(y)], p_s.at[0], p_r.at[b], device(x, t, z)
        )

    def merge_arrival(b):
        return remote(msend.at[b, 0:96], mrecv.at[b, 0:96], p_s.at[0], p_r.at[b], partner)

    def combine(b):
        x_arrival(b).wait_recv()
        rows = xrecv[b]
        total = dot(mixing[b, 0], rows) + dot(mixing[b, 1], rows) + dot(mixing[b, 2], rows)
        msend[b] = total.astype(BF16)
        for d in (2, 1, 3):
            merge_message(b, d).start()
        mrecv[b, part(y), :] = msend[b, part(y), :]

    def home(b):
        return remote(fsend.at[b], frecv.at[z], f_s.at[0], f_r.at[0], device(x, y, along_z(offset(b))))

    def merge(b):
        merge_arrival(b).wait_recv()
        fsend[b] = lax.dot_general(opening[b], mrecv[b], TN, preferred_element_type=F32).astype(BF16)
        if b == 0:
            frecv[z] = fsend[0]
        else:
            home(b).start()

    stages = dict(X=lambda b: own_blocks(), T=tables, U=spread, R=relay, S=select, E=expert, C=combine, M=merge)
    for name in " ".join(ORDER).split():
        run, n = stages[name[0]], int(name[1])
        run(n)

    homes = remote(fsend.at[0 : Z - 1], frecv.at[0 : Z - 1], f_s.at[0], f_r.at[0], partner)
    homes.wait_recv()
    total = frecv[0].astype(F32)
    for i in range(1, Z):
        total = total + frecv[i].astype(F32)
    out[...] = total.astype(BF16)

    def left(send, shape_of):
        remote(shape_of, shape_of, send, f_r.at[0], partner).wait_send()

    left(mi_s.at[0], meta_in.at[0:6])
    left(m_s.at[0], meta.at[0:7])

    @pl.when(c == 0)
    def _():
        left(zs.at[0], slab.at[0:7])
        left(xs.at[0], slab.at[0, 0:192])

    @pl.when(c == 1)
    def _():
        left(zs.at[0], slab.at[0:7, 0:TOK])
        left(xs.at[0], slab.at[0:6])

    gain_give.wait_send()
    for give in gives:
        give.wait_send()
    left(y_s.at[0], ysend.at[:, 0:OTHERS])
    left(x_s.at[0], xsend.at[:, 0:OTHERS])
    left(p_s.at[0], msend.at[:, 0:96])
    homes.wait_send()


def local(tokens, norm_gain, routing, route_weight, w_gate, w_up, w_down):
    vmem = pl.BlockSpec(memory_space=pltpu.VMEM)
    hbm = pl.BlockSpec(memory_space=pltpu.HBM)
    dma = pltpu.SemaphoreType.DMA
    batch = pltpu.VMEM((BATCHES, ROWS, HALF), BF16)
    return pl.pallas_call(
        kernel,
        out_shape=jax.ShapeDtypeStruct((TOK, HALF), BF16),
        in_specs=[hbm] * 7,
        out_specs=vmem,
        scratch_shapes=[
            pltpu.VMEM((TOK, HALF), BF16),
            pltpu.VMEM((1, HALF), F32),
            pltpu.VMEM((2, TOK), jnp.int32),
            pltpu.VMEM((2, TOK), F32),
            pltpu.VMEM((FULL, 2 * HID), BF16),
            pltpu.VMEM((FULL, 2 * HID), BF16),
            pltpu.VMEM((2 * HID, FULL), BF16),
            batch,
            pltpu.VMEM((BATCHES, 16, ROWS), BF16),
            pltpu.VMEM((16, ROWS), BF16),
            pltpu.VMEM((16, ROWS), BF16),
            pltpu.VMEM((8, 16, ROWS), BF16),
            pltpu.VMEM((16, ROWS), F32),
            pltpu.VMEM((ROWS, ROWS), BF16),
            pltpu.VMEM((2, 1, HALF), F32),
            pltpu.VMEM((BATCHES, ROWS, ROWS), BF16),
            pltpu.VMEM((BATCHES, 3, Y * PACK, ROWS), BF16),
            pltpu.VMEM((BATCHES, Y * PACK, TOK), BF16),
            batch,
            batch,
            batch,
            batch,
            pltpu.VMEM((BATCHES, Y * PACK, HALF), BF16),
            pltpu.VMEM((BATCHES, Y * PACK, HALF), BF16),
            pltpu.VMEM((BATCHES, TOK, HALF), BF16),
            pltpu.VMEM((Z, TOK, HALF), BF16),
            dma((4,)),
            dma((3,)),
            dma((3,)),
            dma((3,)),
            dma((2,)),
            dma((BATCHES, X)),
            dma((1,)),
            dma((1,)),
            dma((1,)),
            dma((1,)),
            dma((BATCHES,)),
            dma((1,)),
            dma((1,)),
            dma((BATCHES,)),
            dma((1,)),
            dma((BATCHES,)),
            dma((1,)),
            dma((BATCHES,)),
            dma((1,)),
            dma((1,)),
        ],
        compiler_params=pltpu.CompilerParams(
            collective_id=0, has_side_effects=True, vmem_limit_bytes=60 << 20
        ),
    )(
        tokens, norm_gain.reshape(1, HALF), routing.T.astype(jnp.int32), route_weight.T,
        w_gate, w_up, w_down,
    )


def solution(mesh):
    in_specs = (
        P("ep", "tp"),
        P("tp"),
        P("ep", None),
        P("ep", None),
        P("ep", None, "tp"),
        P("ep", None, "tp"),
        P("ep", None, "tp"),
    )
    return jax.shard_map(
        local, mesh=mesh, in_specs=in_specs, out_specs=P("ep", "tp"), check_vma=False
    )
```

```python
import jax
import jax.numpy as jnp
from jax import lax
from jax.experimental import pallas as pl
from jax.experimental.pallas import tpu as pltpu
from jax.sharding import PartitionSpec as P

F32 = jnp.float32
BF16 = jnp.bfloat16
EPS = 1e-06

X, Y, Z = 4, 4, 8
TOK = 64
HALF = 512
FULL = 1024
HID = 256
SLOTS = 8
BATCHES = 8
ROWS = 256
OTHERS = 224
PACK = 32
LAST = BATCHES - 1

NT = (((1,), (1,)), ((), ()))
TN = (((0,), (0,)), ((), ()))

ORDER = (
    "T0 X0 S0 U1", "U2 T1 T2 R1", "R2 U3 U4 S1", "S2 E0 T3 T4", "U5 U6 U7 R3", "R4 S3 S4 E1",
    "T5 T6 E2 R5", "R6 S5 S6 T7", "E3 R7 S7 C0", "E4 C1 E5 C2", "E6 C3 M0 C4", "E7 M1 M2 C5",
    "M3 C6 M4 M5", "C7 M6 M7",
)
FIRST = 0


def dot(a, b):
    return jnp.dot(a, b, preferred_element_type=F32)


def iota(shape, dim):
    return lax.broadcasted_iota(jnp.int32, shape, dim)


def rem(a, n):
    return lax.rem(a, jnp.int32(n))


def kernel(
    tok_hbm, gain_hbm, picks_hbm, pick_w_hbm, wg_hbm, wu_hbm, wd_hbm, out,
    tok, gain, picks, pick_w, wg, wu, wd, slab, meta, meta_x, meta_y, meta_in, meta_f, tri,
    gains, chosen, mixing, opening, ysend, yrecv, xsend, xrecv, msend, mrecv, fsend, frecv,
    in_sem, w_sem, w_s, w_r, g_sem, slab_r, zs, xs, mi_r, mi_s, m_r, m_s,
    y_s, y_r, x_s, x_r, p_s, p_r, f_s, f_r,
):
    ep = lax.axis_index("ep")
    c = lax.axis_index("tp")
    x = rem(ep, X)
    y = rem(ep // X, Y)
    z = ep // (X * Y)
    group = z * Y + y

    def device(xx, yy, zz, cc=c):
        return (zz * (X * Y) + yy * X + xx, cc)

    def remote(src, dst, send, recv, to):
        return pltpu.make_async_remote_copy(
            src_ref=src, dst_ref=dst, send_sem=send, recv_sem=recv,
            device_id=to, device_id_type=pl.DeviceIdType.MESH,
        )

    def along_x(d):
        return rem(x + d, X)

    def along_y(d):
        return rem(y + d, Y)

    def along_z(d):
        return rem(z + d + Z, Z)

    def core(k):
        return rem(c + k, 2)

    def offset(b):
        return (1 - 2 * (b % 2)) * ((b + 1) // 2)

    partner = (ep, 1 - c)
    barrier = pltpu.get_barrier_semaphore()

    def greet(to):
        pl.semaphore_signal(barrier, inc=1, device_id=to, device_id_type=pl.DeviceIdType.MESH)

    for d in (4, 3, 5, 2, 6, 1, 7):
        greet(device(x, y, along_z(d)))
    for d in (2, 1, 3):
        for k in range(2):
            greet(device(along_x(d), y, z, core(k)))
            greet(device(x, along_y(d), z, core(k)))
    greet(partner)

    inputs = [
        pltpu.make_async_copy(hbm, vmem, in_sem.at[i])
        for i, (hbm, vmem) in enumerate(
            ((picks_hbm, picks), (pick_w_hbm, pick_w), (tok_hbm, tok), (gain_hbm, gain))
        )
    ]
    for copy in inputs:
        copy.start()

    loads = [
        pltpu.make_async_copy(hbm.at[c], vmem.at[:, pl.ds(pl.multiple_of(c * n, n), n)], w_sem.at[i])
        for i, (hbm, vmem, n) in enumerate(((wg_hbm, wg, HID), (wu_hbm, wu, HID), (wd_hbm, wd, HALF)))
    ]
    gives = [
        remote(hbm.at[1 - c], vmem.at[:, pl.ds(pl.multiple_of(c * n, n), n)], w_s.at[i], w_r.at[i], partner)
        for i, (hbm, vmem, n) in enumerate(((wg_hbm, wg, HID), (wu_hbm, wu, HID), (wd_hbm, wd, HALF)))
    ]
    takes = [
        remote(hbm.at[c], vmem.at[:, pl.ds(pl.multiple_of((1 - c) * n, n), n)], w_s.at[i], w_r.at[i], partner)
        for i, (hbm, vmem, n) in enumerate(((wg_hbm, wg, HID), (wu_hbm, wu, HID), (wd_hbm, wd, HALF)))
    ]
    for load in loads:
        load.start()

    for copy in inputs:
        copy.wait()
    lanes = iota((TOK, ROWS), 1) - iota((TOK, ROWS), 0)
    at_x = jnp.where(lanes == x * TOK, 1.0, 0.0).astype(BF16)
    at_y = jnp.where(lanes == y * TOK, 1.0, 0.0).astype(BF16)
    names = picks[...].astype(F32).astype(BF16)
    weight = pick_w[...]
    hi = weight.astype(BF16)
    rest = weight - hi.astype(F32)
    mid = rest.astype(BF16)
    low = (rest - mid.astype(F32)).astype(BF16)
    meta_f[...] = jnp.zeros((16, ROWS), F32)
    meta_f[8:10, :] = dot(names, at_x)
    meta_x[...] = meta_f[...].astype(BF16)
    meta_f[8:10, :] = jnp.zeros((2, ROWS), F32)
    for k, part in enumerate((names, hi, mid, low)):
        meta_f[2 * k : 2 * k + 2, :] = dot(part, at_y)
    meta_y[...] = meta_f[...].astype(BF16)
    a, b = iota((ROWS, ROWS), 0), iota((ROWS, ROWS), 1)
    tri[...] = jnp.where((a // TOK == b // TOK) & (a < b), 1.0, 0.0).astype(BF16)
    slab[0, pl.ds(pl.multiple_of(x * TOK, TOK), TOK), :] = tok[...]
    gains[c] = gain[...]

    def block(b, s):
        return slab.at[b, pl.ds(pl.multiple_of(s * TOK, TOK), TOK)]

    def own_to_x(d):
        return remote(tok, block(0, x), xs.at[0], slab_r.at[0, x], device(along_x(d), y, z))

    def from_x(d):
        s = along_x(d)
        return remote(tok, block(0, s), xs.at[0], slab_r.at[0, s], device(s, y, z))

    def along(b, to, s, sign):
        return remote(
            block(b, s), block(to, s), zs.at[0], slab_r.at[to, s], device(x, y, along_z(sign))
        )

    def own_along(to, sign):
        return remote(tok, block(to, x), zs.at[0], slab_r.at[to, x], device(x, y, along_z(sign)))

    def meta_along(b, to, sign):
        return remote(meta.at[b], meta.at[to], m_s.at[0], m_r.at[to], device(x, y, along_z(sign)))

    def meta_to_x(d):
        return remote(meta_x, meta_in.at[x], mi_s.at[0], mi_r.at[0], device(along_x(d), y, z))

    def meta_to_y(d):
        return remote(meta_y, meta_in.at[X + y], mi_s.at[0], mi_r.at[0], device(x, along_y(d), z))

    meta_all = remote(meta_in.at[0:6], meta_in.at[0:6], mi_s.at[0], mi_r.at[0], partner)

    gain_give = remote(gain, gains.at[c], g_sem.at[0], g_sem.at[1], partner)
    gain_take = remote(gain, gains.at[1 - c], g_sem.at[0], g_sem.at[1], partner)

    pl.semaphore_wait(barrier, (Z - 1) + 2 * (X - 1) + 2 * (Y - 1) + 1)

    for d in (2, 1, 3):
        meta_to_x(d).start()
        meta_to_y(d).start()
    for d in (2, 1, 3):
        own_to_x(d).start()
    @pl.when(c == 0)
    def _():
        own_along(1, 1).start()
        own_along(2, -1).start()

    @pl.when(c == 1)
    def _():
        for b in range(1, BATCHES):
            own_along(b, -offset(b)).start()

    gain_give.start()

    meta_all.wait_recv()
    table = meta_x[...].astype(F32) + meta_y[...].astype(F32)
    for d in range(1, 4):
        table = table + meta_in[along_x(d)].astype(F32) + meta_in[X + along_y(d)].astype(F32)
    meta[0] = table.astype(BF16)
    meta_along(0, 1, 1).start()
    meta_along(0, 2, -1).start()

    def own_blocks():
        for d in (1, 3, 2):
            own_block(d)
        for give in gives:
            give.start()

    def own_block(d):
        from_x(d).wait_recv()

        @pl.when(c == 0)
        def _():
            s = along_x(d)
            along(0, 1, s, 1).start()
            along(0, 2, s, -1).start()

    def block_to_x(b, d):
        return remote(block(b, x), block(b, x), xs.at[0], slab_r.at[b, x], device(along_x(d), y, z))

    def tables(b):
        if b > 0:
            sign = 1 if b % 2 else -1
            meta_along(b, b, sign).wait_recv()
            if b <= 5:
                meta_along(b, b + 2, sign).start()
        prepare(b)

    def relay(b):
        sign = 1 if b % 2 else -1
        to = min(b + 2, LAST)

        @pl.when(c == 0)
        def _():
            for s in range(X):
                along(b, b, s, sign).wait_recv()
                if b <= 4 or (b == 5 and s < 2) or (b == 6 and s >= 2):
                    along(b, to, s, sign).start()

    def spread(b):
        @pl.when(c == 1)
        def _():
            along(b, b, x, 1).wait_recv()
            for d in (2, 1, 3):
                block_to_x(b, d).start()

    def gathered(b):
        if b == 0:
            return

        @pl.when(c == 1)
        def _():
            for d in (1, 3, 2):
                s = along_x(d)
                remote(block(b, s), block(b, s), xs.at[0], slab_r.at[b, s], device(s, y, z)).wait_recv()

    def part(i):
        return pl.ds(pl.multiple_of(i * PACK, PACK), PACK)

    PEERS = [(d, k) for d in (2, 1, 3, 0) for k in (0, 1) if (d, k) != (0, 0)]

    def y_message(b, d, k):
        t, j = along_y(d), core(k)
        return remote(
            ysend.at[b, part(t * 2 + j)], yrecv.at[b, part(c * Y + y)],
            y_s.at[0], y_r.at[b], device(x, t, z, j),
        )

    def y_arrival(b):
        return remote(ysend.at[b, 0:OTHERS], yrecv.at[b, 0:OTHERS], y_s.at[0], y_r.at[b], partner)

    row = iota((8, ROWS), 0)
    segment = (iota((8, ROWS), 1) // TOK).astype(F32)
    slot = iota((PACK, ROWS), 0).astype(F32)

    def spread_out(code, value):
        return jnp.concatenate(
            [jnp.where(code[q : q + 1, :] == slot, value[q : q + 1, :], 0.0) for q in range(8)], axis=0
        ).astype(BF16)

    def prepare(b):
        table = meta[b].astype(F32)
        expert = (z * 32 + row // 2 * 8 + x * 2 + rem(row, 2)).astype(F32)
        hit = jnp.where((table[8:9, :] == expert) | (table[9:10, :] == expert), 1.0, 0.0)
        member = (group * 8 + row).astype(F32)
        first, second = table[0:1, :] == member, table[1:2, :] == member
        hit_here = jnp.where(first | second, 1.0, 0.0)
        low = ((z * Y + row) * 8).astype(F32)
        hit_z = jnp.where((table[0:1, :] >= low) & (table[0:1, :] < low + 8.0) & (row < Y), 1.0, 0.0)
        ranks = dot(jnp.concatenate([hit, hit_here, hit_z, hit_z], axis=0).astype(BF16), tri[...])
        chosen[b] = spread_out(
            jnp.where(hit > 0.0, segment * SLOTS + ranks[0:8, :], -1.0), jnp.ones((8, ROWS), F32)
        )
        code = jnp.where(hit_here > 0.0, segment * SLOTS + ranks[8:16, :], -1.0)
        rank_z = jnp.where(hit_z > 0.0, ranks[16:24, :], -1.0)
        spot = jnp.sum(
            jnp.where((row == y) & (hit_z > 0.0), segment * PACK + ranks[16:24, :] + 1.0, 0.0), axis=0, keepdims=True
        )
        packing = jnp.where(spot - 1.0 == iota((Y * PACK, ROWS), 0).astype(F32), 1.0, 0.0).astype(BF16)
        for k in range(1, 4):
            value = jnp.where(first, table[2 * k : 2 * k + 1, :], 0.0) + jnp.where(
                second, table[2 * k + 1 : 2 * k + 2, :], 0.0
            )
            mixing[b, k - 1] = lax.dot_general(
                packing, spread_out(code, value), NT, preferred_element_type=F32
            ).astype(BF16)
        mine = jnp.where(iota((ROWS, TOK), 0) - iota((ROWS, TOK), 1) == y * TOK, 1.0, 0.0).astype(BF16)
        own = dot(rank_z.astype(BF16), mine)
        spots = iota((PACK, TOK), 0).astype(F32)
        opening[b] = jnp.concatenate(
            [jnp.where(own[q : q + 1, :] == spots, 1.0, 0.0) for q in range(Y)], axis=0
        ).astype(BF16)

    def select(b):
        gathered(b)
        ysend[b] = dot(chosen[b], slab[b]).astype(BF16)
        for d, k in PEERS:
            y_message(b, d, k).start()
        yrecv[b, part(c * Y + y), :] = ysend[b, part(y * 2 + c), :]

    def x_message(b, d, k):
        t, h = along_x(d), core(k)
        return remote(
            xsend.at[b, part(t * 2 + h)], xrecv.at[b, part(x * 2 + c)],
            x_s.at[0], x_r.at[b], device(t, y, z, h),
        )

    def x_arrival(b):
        return remote(xsend.at[b, 0:OTHERS], xrecv.at[b, 0:OTHERS], x_s.at[0], x_r.at[b], partner)

    def expert(b):
        y_arrival(b).wait_recv()

        if b == FIRST:
            gain_take.wait_recv()
            for load in loads:
                load.wait()
            for take in takes:
                take.wait_recv()

        low, high = yrecv[b, 0:128, :].astype(F32), yrecv[b, 128:256, :].astype(F32)
        total = jnp.sum(low * low, axis=1, keepdims=True) + jnp.sum(high * high, axis=1, keepdims=True)
        scale = lax.rsqrt(total / FULL + EPS)
        rows = jnp.concatenate(
            [(low * scale * gains[0]).astype(BF16), (high * scale * gains[1]).astype(BF16)], axis=1
        )
        gate = dot(rows, wg[...])
        up = dot(rows, wu[...])
        hidden = (gate / (1.0 + jnp.exp(-gate)) * up).astype(BF16)
        result = dot(hidden, wd[...])
        for t in range(X):
            piece = jnp.concatenate(
                [result[(s * X + t) * 8 : (s * X + t) * 8 + 8, :] for s in range(Y)], axis=0
            ).astype(BF16)
            for h in range(2):
                xsend[b, (t * 2 + h) * PACK : (t * 2 + h + 1) * PACK, :] = piece[:, h * HALF : (h + 1) * HALF]
        for d, k in PEERS:
            x_message(b, d, k).start()
        xrecv[b, part(x * 2 + c), :] = xsend[b, part(x * 2 + c), :]

    def merge_message(b, d):
        t = along_y(d)
        return remote(
            msend.at[b, part(t)], mrecv.at[b, part(y)], p_s.at[0], p_r.at[b], device(x, t, z)
        )

    def merge_arrival(b):
        return remote(msend.at[b, 0:96], mrecv.at[b, 0:96], p_s.at[0], p_r.at[b], partner)

    def combine(b):
        x_arrival(b).wait_recv()
        rows = xrecv[b]
        total = dot(mixing[b, 0], rows) + dot(mixing[b, 1], rows) + dot(mixing[b, 2], rows)
        msend[b] = total.astype(BF16)
        for d in (2, 1, 3):
            merge_message(b, d).start()
        mrecv[b, part(y), :] = msend[b, part(y), :]

    def home(b):
        return remote(fsend.at[b], frecv.at[z], f_s.at[0], f_r.at[0], device(x, y, along_z(offset(b))))

    def merge(b):
        merge_arrival(b).wait_recv()
        fsend[b] = lax.dot_general(opening[b], mrecv[b], TN, preferred_element_type=F32).astype(BF16)
        if b == 0:
            frecv[z] = fsend[0]
        else:
            home(b).start()

    stages = dict(X=lambda b: own_blocks(), T=tables, U=spread, R=relay, S=select, E=expert, C=combine, M=merge)
    for name in " ".join(ORDER).split():
        run, n = stages[name[0]], int(name[1])
        run(n)

    homes = remote(fsend.at[0 : Z - 1], frecv.at[0 : Z - 1], f_s.at[0], f_r.at[0], partner)
    homes.wait_recv()
    total = frecv[0].astype(F32)
    for i in range(1, Z):
        total = total + frecv[i].astype(F32)
    out[...] = total.astype(BF16)

    def left(send, shape_of):
        remote(shape_of, shape_of, send, f_r.at[0], partner).wait_send()

    left(mi_s.at[0], meta_in.at[0:6])
    left(m_s.at[0], meta.at[0:7])

    @pl.when(c == 0)
    def _():
        left(zs.at[0], slab.at[0:7])
        left(xs.at[0], slab.at[0, 0:192])

    @pl.when(c == 1)
    def _():
        left(zs.at[0], slab.at[0:7, 0:TOK])
        left(xs.at[0], slab.at[0:6])

    gain_give.wait_send()
    for give in gives:
        give.wait_send()
    left(y_s.at[0], ysend.at[:, 0:OTHERS])
    left(x_s.at[0], xsend.at[:, 0:OTHERS])
    left(p_s.at[0], msend.at[:, 0:96])
    homes.wait_send()


def local(tokens, norm_gain, routing, route_weight, w_gate, w_up, w_down):
    vmem = pl.BlockSpec(memory_space=pltpu.VMEM)
    hbm = pl.BlockSpec(memory_space=pltpu.HBM)
    dma = pltpu.SemaphoreType.DMA
    batch = pltpu.VMEM((BATCHES, ROWS, HALF), BF16)
    return pl.pallas_call(
        kernel,
        out_shape=jax.ShapeDtypeStruct((TOK, HALF), BF16),
        in_specs=[hbm] * 7,
        out_specs=vmem,
        scratch_shapes=[
            pltpu.VMEM((TOK, HALF), BF16),
            pltpu.VMEM((1, HALF), F32),
            pltpu.VMEM((2, TOK), jnp.int32),
            pltpu.VMEM((2, TOK), F32),
            pltpu.VMEM((FULL, 2 * HID), BF16),
            pltpu.VMEM((FULL, 2 * HID), BF16),
            pltpu.VMEM((2 * HID, FULL), BF16),
            batch,
            pltpu.VMEM((BATCHES, 16, ROWS), BF16),
            pltpu.VMEM((16, ROWS), BF16),
            pltpu.VMEM((16, ROWS), BF16),
            pltpu.VMEM((8, 16, ROWS), BF16),
            pltpu.VMEM((16, ROWS), F32),
            pltpu.VMEM((ROWS, ROWS), BF16),
            pltpu.VMEM((2, 1, HALF), F32),
            pltpu.VMEM((BATCHES, ROWS, ROWS), BF16),
            pltpu.VMEM((BATCHES, 3, Y * PACK, ROWS), BF16),
            pltpu.VMEM((BATCHES, Y * PACK, TOK), BF16),
            batch,
            batch,
            batch,
            batch,
            pltpu.VMEM((BATCHES, Y * PACK, HALF), BF16),
            pltpu.VMEM((BATCHES, Y * PACK, HALF), BF16),
            pltpu.VMEM((BATCHES, TOK, HALF), BF16),
            pltpu.VMEM((Z, TOK, HALF), BF16),
            dma((4,)),
            dma((3,)),
            dma((3,)),
            dma((3,)),
            dma((2,)),
            dma((BATCHES, X)),
            dma((1,)),
            dma((1,)),
            dma((1,)),
            dma((1,)),
            dma((BATCHES,)),
            dma((1,)),
            dma((1,)),
            dma((BATCHES,)),
            dma((1,)),
            dma((BATCHES,)),
            dma((1,)),
            dma((BATCHES,)),
            dma((1,)),
            dma((1,)),
        ],
        compiler_params=pltpu.CompilerParams(
            collective_id=0, has_side_effects=True, vmem_limit_bytes=60 << 20
        ),
    )(
        tokens, norm_gain.reshape(1, HALF), routing.T.astype(jnp.int32), route_weight.T,
        w_gate, w_up, w_down,
    )


def solution(mesh):
    in_specs = (
        P("ep", "tp"),
        P("tp"),
        P("ep", None),
        P("ep", None),
        P("ep", None, "tp"),
        P("ep", None, "tp"),
        P("ep", None, "tp"),
    )
    return jax.shard_map(
        local, mesh=mesh, in_specs=in_specs, out_specs=P("ep", "tp"), check_vma=False
    )
```

```python
import jax
import jax.numpy as jnp
from jax import lax
from jax.experimental import pallas as pl
from jax.experimental.pallas import tpu as pltpu
from jax.sharding import PartitionSpec as P

F32 = jnp.float32
BF16 = jnp.bfloat16
EPS = 1e-06

X, Y, Z = 4, 4, 8
TOK = 64
HALF = 512
FULL = 1024
HID = 256
SLOTS = 8
BATCHES = 8
ROWS = 256
OTHERS = 224
PACK = 32
LAST = BATCHES - 1

NT = (((1,), (1,)), ((), ()))
TN = (((0,), (0,)), ((), ()))

ORDER = (
    "T0 X0 S0 U1", "U2 T1 T2 R1", "R2 U3 U4 S1", "S2 E0 T3 T4", "U5 U6 U7 R3", "R4 S3 S4 E1",
    "T5 T6 E2 R5", "R6 S5 S6 T7", "E3 R7 S7 C0", "E4 C1 E5 C2", "E6 C3 M0 C4", "E7 M1 M2 C5",
    "M3 C6 M4 M5", "C7 M6 M7",
)
FIRST = 0


def dot(a, b):
    return jnp.dot(a, b, preferred_element_type=F32)


def iota(shape, dim):
    return lax.broadcasted_iota(jnp.int32, shape, dim)


def rem(a, n):
    return lax.rem(a, jnp.int32(n))


def kernel(
    tok_hbm, gain_hbm, picks_hbm, pick_w_hbm, wg_hbm, wu_hbm, wd_hbm, out,
    tok, gain, picks, pick_w, wg, wu, wd, slab, meta, meta_x, meta_y, meta_in, meta_f, tri,
    gains, chosen, mixing, opening, ysend, yrecv, xsend, xrecv, msend, mrecv, fsend, frecv,
    in_sem, w_sem, w_s, w_r, g_sem, slab_r, zs, xs, mi_r, mi_s, m_r, m_s,
    y_s, y_r, x_s, x_r, p_s, p_r, f_s, f_r,
):
    ep = lax.axis_index("ep")
    c = lax.axis_index("tp")
    x = rem(ep, X)
    y = rem(ep // X, Y)
    z = ep // (X * Y)
    group = z * Y + y

    def device(xx, yy, zz, cc=c):
        return (zz * (X * Y) + yy * X + xx, cc)

    def remote(src, dst, send, recv, to):
        return pltpu.make_async_remote_copy(
            src_ref=src, dst_ref=dst, send_sem=send, recv_sem=recv,
            device_id=to, device_id_type=pl.DeviceIdType.MESH,
        )

    def along_x(d):
        return rem(x + d, X)

    def along_y(d):
        return rem(y + d, Y)

    def along_z(d):
        return rem(z + d + Z, Z)

    def core(k):
        return rem(c + k, 2)

    def offset(b):
        return (1 - 2 * (b % 2)) * ((b + 1) // 2)

    partner = (ep, 1 - c)
    barrier = pltpu.get_barrier_semaphore()

    def greet(to):
        pl.semaphore_signal(barrier, inc=1, device_id=to, device_id_type=pl.DeviceIdType.MESH)

    for d in (4, 3, 5, 2, 6, 1, 7):
        greet(device(x, y, along_z(d)))
    for d in (2, 1, 3):
        for k in range(2):
            greet(device(along_x(d), y, z, core(k)))
            greet(device(x, along_y(d), z, core(k)))
    greet(partner)

    inputs = [
        pltpu.make_async_copy(hbm, vmem, in_sem.at[i])
        for i, (hbm, vmem) in enumerate(
            ((picks_hbm, picks), (pick_w_hbm, pick_w), (tok_hbm, tok), (gain_hbm, gain))
        )
    ]
    for copy in inputs:
        copy.start()

    loads = [
        pltpu.make_async_copy(hbm.at[c], vmem.at[:, pl.ds(pl.multiple_of(c * n, n), n)], w_sem.at[i])
        for i, (hbm, vmem, n) in enumerate(((wg_hbm, wg, HID), (wu_hbm, wu, HID), (wd_hbm, wd, HALF)))
    ]
    gives = [
        remote(hbm.at[1 - c], vmem.at[:, pl.ds(pl.multiple_of(c * n, n), n)], w_s.at[i], w_r.at[i], partner)
        for i, (hbm, vmem, n) in enumerate(((wg_hbm, wg, HID), (wu_hbm, wu, HID), (wd_hbm, wd, HALF)))
    ]
    takes = [
        remote(hbm.at[c], vmem.at[:, pl.ds(pl.multiple_of((1 - c) * n, n), n)], w_s.at[i], w_r.at[i], partner)
        for i, (hbm, vmem, n) in enumerate(((wg_hbm, wg, HID), (wu_hbm, wu, HID), (wd_hbm, wd, HALF)))
    ]
    for load in loads:
        load.start()

    for copy in inputs:
        copy.wait()
    lanes = iota((TOK, ROWS), 1) - iota((TOK, ROWS), 0)
    at_x = jnp.where(lanes == x * TOK, 1.0, 0.0).astype(BF16)
    at_y = jnp.where(lanes == y * TOK, 1.0, 0.0).astype(BF16)
    names = picks[...].astype(F32).astype(BF16)
    weight = pick_w[...]
    hi = weight.astype(BF16)
    rest = weight - hi.astype(F32)
    mid = rest.astype(BF16)
    low = (rest - mid.astype(F32)).astype(BF16)
    meta_f[...] = jnp.zeros((16, ROWS), F32)
    meta_f[8:10, :] = dot(names, at_x)
    meta_x[...] = meta_f[...].astype(BF16)
    meta_f[8:10, :] = jnp.zeros((2, ROWS), F32)
    for k, part in enumerate((names, hi, mid, low)):
        meta_f[2 * k : 2 * k + 2, :] = dot(part, at_y)
    meta_y[...] = meta_f[...].astype(BF16)
    a, b = iota((ROWS, ROWS), 0), iota((ROWS, ROWS), 1)
    tri[...] = jnp.where((a // TOK == b // TOK) & (a < b), 1.0, 0.0).astype(BF16)
    slab[0, pl.ds(pl.multiple_of(x * TOK, TOK), TOK), :] = tok[...]
    gains[c] = gain[...]

    def block(b, s):
        return slab.at[b, pl.ds(pl.multiple_of(s * TOK, TOK), TOK)]

    def own_to_x(d):
        return remote(tok, block(0, x), xs.at[0], slab_r.at[0, x], device(along_x(d), y, z))

    def from_x(d):
        s = along_x(d)
        return remote(tok, block(0, s), xs.at[0], slab_r.at[0, s], device(s, y, z))

    def along(b, to, s, sign):
        return remote(
            block(b, s), block(to, s), zs.at[0], slab_r.at[to, s], device(x, y, along_z(sign))
        )

    def own_along(to, sign):
        return remote(tok, block(to, x), zs.at[0], slab_r.at[to, x], device(x, y, along_z(sign)))

    def meta_along(b, to, sign):
        return remote(meta.at[b], meta.at[to], m_s.at[0], m_r.at[to], device(x, y, along_z(sign)))

    def meta_to_x(d):
        return remote(meta_x, meta_in.at[x], mi_s.at[0], mi_r.at[0], device(along_x(d), y, z))

    def meta_to_y(d):
        return remote(meta_y, meta_in.at[X + y], mi_s.at[0], mi_r.at[0], device(x, along_y(d), z))

    meta_all = remote(meta_in.at[0:6], meta_in.at[0:6], mi_s.at[0], mi_r.at[0], partner)

    gain_give = remote(gain, gains.at[c], g_sem.at[0], g_sem.at[1], partner)
    gain_take = remote(gain, gains.at[1 - c], g_sem.at[0], g_sem.at[1], partner)

    pl.semaphore_wait(barrier, (Z - 1) + 2 * (X - 1) + 2 * (Y - 1) + 1)

    for d in (2, 1, 3):
        meta_to_x(d).start()
        meta_to_y(d).start()
    for d in (2, 1, 3):
        own_to_x(d).start()
    @pl.when(c == 0)
    def _():
        own_along(1, 1).start()
        own_along(2, -1).start()

    @pl.when(c == 1)
    def _():
        for b in range(1, BATCHES):
            own_along(b, -offset(b)).start()

    gain_give.start()

    meta_all.wait_recv()
    table = meta_x[...].astype(F32) + meta_y[...].astype(F32)
    for d in range(1, 4):
        table = table + meta_in[along_x(d)].astype(F32) + meta_in[X + along_y(d)].astype(F32)
    meta[0] = table.astype(BF16)
    meta_along(0, 1, 1).start()
    meta_along(0, 2, -1).start()

    def own_blocks():
        for d in (1, 3, 2):
            own_block(d)

    def own_block(d):
        from_x(d).wait_recv()

        @pl.when(c == 0)
        def _():
            s = along_x(d)
            along(0, 1, s, 1).start()
            along(0, 2, s, -1).start()

    def block_to_x(b, d):
        return remote(block(b, x), block(b, x), xs.at[0], slab_r.at[b, x], device(along_x(d), y, z))

    def tables(b):
        if b > 0:
            sign = 1 if b % 2 else -1
            meta_along(b, b, sign).wait_recv()
            if b <= 5:
                meta_along(b, b + 2, sign).start()
        if b == 1:
            for give in gives:
                give.start()
        prepare(b)

    def relay(b):
        sign = 1 if b % 2 else -1
        to = min(b + 2, LAST)

        @pl.when(c == 0)
        def _():
            for s in range(X):
                along(b, b, s, sign).wait_recv()
                if b <= 4 or (b == 5 and s < 2) or (b == 6 and s >= 2):
                    along(b, to, s, sign).start()

    def spread(b):
        @pl.when(c == 1)
        def _():
            along(b, b, x, 1).wait_recv()
            for d in (2, 1, 3):
                block_to_x(b, d).start()

    def gathered(b):
        if b == 0:
            return

        @pl.when(c == 1)
        def _():
            for d in (1, 3, 2):
                s = along_x(d)
                remote(block(b, s), block(b, s), xs.at[0], slab_r.at[b, s], device(s, y, z)).wait_recv()

    def part(i):
        return pl.ds(pl.multiple_of(i * PACK, PACK), PACK)

    PEERS = [(d, k) for d in (2, 1, 3, 0) for k in (0, 1) if (d, k) != (0, 0)]

    def y_message(b, d, k):
        t, j = along_y(d), core(k)
        return remote(
            ysend.at[b, part(t * 2 + j)], yrecv.at[b, part(c * Y + y)],
            y_s.at[0], y_r.at[b], device(x, t, z, j),
        )

    def y_arrival(b):
        return remote(ysend.at[b, 0:OTHERS], yrecv.at[b, 0:OTHERS], y_s.at[0], y_r.at[b], partner)

    row = iota((8, ROWS), 0)
    segment = (iota((8, ROWS), 1) // TOK).astype(F32)
    slot = iota((PACK, ROWS), 0).astype(F32)

    def spread_out(code, value):
        return jnp.concatenate(
            [jnp.where(code[q : q + 1, :] == slot, value[q : q + 1, :], 0.0) for q in range(8)], axis=0
        ).astype(BF16)

    def prepare(b):
        table = meta[b].astype(F32)
        expert = (z * 32 + row // 2 * 8 + x * 2 + rem(row, 2)).astype(F32)
        hit = jnp.where((table[8:9, :] == expert) | (table[9:10, :] == expert), 1.0, 0.0)
        member = (group * 8 + row).astype(F32)
        first, second = table[0:1, :] == member, table[1:2, :] == member
        hit_here = jnp.where(first | second, 1.0, 0.0)
        low = ((z * Y + row) * 8).astype(F32)
        hit_z = jnp.where((table[0:1, :] >= low) & (table[0:1, :] < low + 8.0) & (row < Y), 1.0, 0.0)
        ranks = dot(jnp.concatenate([hit, hit_here, hit_z, hit_z], axis=0).astype(BF16), tri[...])
        chosen[b] = spread_out(
            jnp.where(hit > 0.0, segment * SLOTS + ranks[0:8, :], -1.0), jnp.ones((8, ROWS), F32)
        )
        code = jnp.where(hit_here > 0.0, segment * SLOTS + ranks[8:16, :], -1.0)
        rank_z = jnp.where(hit_z > 0.0, ranks[16:24, :], -1.0)
        spot = jnp.sum(
            jnp.where((row == y) & (hit_z > 0.0), segment * PACK + ranks[16:24, :] + 1.0, 0.0), axis=0, keepdims=True
        )
        packing = jnp.where(spot - 1.0 == iota((Y * PACK, ROWS), 0).astype(F32), 1.0, 0.0).astype(BF16)
        for k in range(1, 4):
            value = jnp.where(first, table[2 * k : 2 * k + 1, :], 0.0) + jnp.where(
                second, table[2 * k + 1 : 2 * k + 2, :], 0.0
            )
            mixing[b, k - 1] = lax.dot_general(
                packing, spread_out(code, value), NT, preferred_element_type=F32
            ).astype(BF16)
        mine = jnp.where(iota((ROWS, TOK), 0) - iota((ROWS, TOK), 1) == y * TOK, 1.0, 0.0).astype(BF16)
        own = dot(rank_z.astype(BF16), mine)
        spots = iota((PACK, TOK), 0).astype(F32)
        opening[b] = jnp.concatenate(
            [jnp.where(own[q : q + 1, :] == spots, 1.0, 0.0) for q in range(Y)], axis=0
        ).astype(BF16)

    def select(b):
        gathered(b)
        ysend[b] = dot(chosen[b], slab[b]).astype(BF16)
        for d, k in PEERS:
            y_message(b, d, k).start()
        yrecv[b, part(c * Y + y), :] = ysend[b, part(y * 2 + c), :]

    def x_message(b, d, k):
        t, h = along_x(d), core(k)
        return remote(
            xsend.at[b, part(t * 2 + h)], xrecv.at[b, part(x * 2 + c)],
            x_s.at[0], x_r.at[b], device(t, y, z, h),
        )

    def x_arrival(b):
        return remote(xsend.at[b, 0:OTHERS], xrecv.at[b, 0:OTHERS], x_s.at[0], x_r.at[b], partner)

    def expert(b):
        y_arrival(b).wait_recv()

        if b == FIRST:
            gain_take.wait_recv()
            for load in loads:
                load.wait()
            for take in takes:
                take.wait_recv()

        low, high = yrecv[b, 0:128, :].astype(F32), yrecv[b, 128:256, :].astype(F32)
        total = jnp.sum(low * low, axis=1, keepdims=True) + jnp.sum(high * high, axis=1, keepdims=True)
        scale = lax.rsqrt(total / FULL + EPS)
        rows = jnp.concatenate(
            [(low * scale * gains[0]).astype(BF16), (high * scale * gains[1]).astype(BF16)], axis=1
        )
        gate = dot(rows, wg[...])
        up = dot(rows, wu[...])
        hidden = (gate / (1.0 + jnp.exp(-gate)) * up).astype(BF16)
        result = dot(hidden, wd[...])
        for t in range(X):
            piece = jnp.concatenate(
                [result[(s * X + t) * 8 : (s * X + t) * 8 + 8, :] for s in range(Y)], axis=0
            ).astype(BF16)
            for h in range(2):
                xsend[b, (t * 2 + h) * PACK : (t * 2 + h + 1) * PACK, :] = piece[:, h * HALF : (h + 1) * HALF]
        for d, k in PEERS:
            x_message(b, d, k).start()
        xrecv[b, part(x * 2 + c), :] = xsend[b, part(x * 2 + c), :]

    def merge_message(b, d):
        t = along_y(d)
        return remote(
            msend.at[b, part(t)], mrecv.at[b, part(y)], p_s.at[0], p_r.at[b], device(x, t, z)
        )

    def merge_arrival(b):
        return remote(msend.at[b, 0:96], mrecv.at[b, 0:96], p_s.at[0], p_r.at[b], partner)

    def combine(b):
        x_arrival(b).wait_recv()
        rows = xrecv[b]
        total = dot(mixing[b, 0], rows) + dot(mixing[b, 1], rows) + dot(mixing[b, 2], rows)
        msend[b] = total.astype(BF16)
        for d in (2, 1, 3):
            merge_message(b, d).start()
        mrecv[b, part(y), :] = msend[b, part(y), :]

    def home(b):
        return remote(fsend.at[b], frecv.at[z], f_s.at[0], f_r.at[0], device(x, y, along_z(offset(b))))

    def merge(b):
        merge_arrival(b).wait_recv()
        fsend[b] = lax.dot_general(opening[b], mrecv[b], TN, preferred_element_type=F32).astype(BF16)
        if b == 0:
            frecv[z] = fsend[0]
        else:
            home(b).start()

    stages = dict(X=lambda b: own_blocks(), T=tables, U=spread, R=relay, S=select, E=expert, C=combine, M=merge)
    for name in " ".join(ORDER).split():
        run, n = stages[name[0]], int(name[1])
        run(n)

    homes = remote(fsend.at[0 : Z - 1], frecv.at[0 : Z - 1], f_s.at[0], f_r.at[0], partner)
    homes.wait_recv()
    total = frecv[0].astype(F32)
    for i in range(1, Z):
        total = total + frecv[i].astype(F32)
    out[...] = total.astype(BF16)

    def left(send, shape_of):
        remote(shape_of, shape_of, send, f_r.at[0], partner).wait_send()

    left(mi_s.at[0], meta_in.at[0:6])
    left(m_s.at[0], meta.at[0:7])

    @pl.when(c == 0)
    def _():
        left(zs.at[0], slab.at[0:7])
        left(xs.at[0], slab.at[0, 0:192])

    @pl.when(c == 1)
    def _():
        left(zs.at[0], slab.at[0:7, 0:TOK])
        left(xs.at[0], slab.at[0:6])

    gain_give.wait_send()
    for give in gives:
        give.wait_send()
    left(y_s.at[0], ysend.at[:, 0:OTHERS])
    left(x_s.at[0], xsend.at[:, 0:OTHERS])
    left(p_s.at[0], msend.at[:, 0:96])
    homes.wait_send()


def local(tokens, norm_gain, routing, route_weight, w_gate, w_up, w_down):
    vmem = pl.BlockSpec(memory_space=pltpu.VMEM)
    hbm = pl.BlockSpec(memory_space=pltpu.HBM)
    dma = pltpu.SemaphoreType.DMA
    batch = pltpu.VMEM((BATCHES, ROWS, HALF), BF16)
    return pl.pallas_call(
        kernel,
        out_shape=jax.ShapeDtypeStruct((TOK, HALF), BF16),
        in_specs=[hbm] * 7,
        out_specs=vmem,
        scratch_shapes=[
            pltpu.VMEM((TOK, HALF), BF16),
            pltpu.VMEM((1, HALF), F32),
            pltpu.VMEM((2, TOK), jnp.int32),
            pltpu.VMEM((2, TOK), F32),
            pltpu.VMEM((FULL, 2 * HID), BF16),
            pltpu.VMEM((FULL, 2 * HID), BF16),
            pltpu.VMEM((2 * HID, FULL), BF16),
            batch,
            pltpu.VMEM((BATCHES, 16, ROWS), BF16),
            pltpu.VMEM((16, ROWS), BF16),
            pltpu.VMEM((16, ROWS), BF16),
            pltpu.VMEM((8, 16, ROWS), BF16),
            pltpu.VMEM((16, ROWS), F32),
            pltpu.VMEM((ROWS, ROWS), BF16),
            pltpu.VMEM((2, 1, HALF), F32),
            pltpu.VMEM((BATCHES, ROWS, ROWS), BF16),
            pltpu.VMEM((BATCHES, 3, Y * PACK, ROWS), BF16),
            pltpu.VMEM((BATCHES, Y * PACK, TOK), BF16),
            batch,
            batch,
            batch,
            batch,
            pltpu.VMEM((BATCHES, Y * PACK, HALF), BF16),
            pltpu.VMEM((BATCHES, Y * PACK, HALF), BF16),
            pltpu.VMEM((BATCHES, TOK, HALF), BF16),
            pltpu.VMEM((Z, TOK, HALF), BF16),
            dma((4,)),
            dma((3,)),
            dma((3,)),
            dma((3,)),
            dma((2,)),
            dma((BATCHES, X)),
            dma((1,)),
            dma((1,)),
            dma((1,)),
            dma((1,)),
            dma((BATCHES,)),
            dma((1,)),
            dma((1,)),
            dma((BATCHES,)),
            dma((1,)),
            dma((BATCHES,)),
            dma((1,)),
            dma((BATCHES,)),
            dma((1,)),
            dma((1,)),
        ],
        compiler_params=pltpu.CompilerParams(
            collective_id=0, has_side_effects=True, vmem_limit_bytes=60 << 20
        ),
    )(
        tokens, norm_gain.reshape(1, HALF), routing.T.astype(jnp.int32), route_weight.T,
        w_gate, w_up, w_down,
    )


def solution(mesh):
    in_specs = (
        P("ep", "tp"),
        P("tp"),
        P("ep", None),
        P("ep", None),
        P("ep", None, "tp"),
        P("ep", None, "tp"),
        P("ep", None, "tp"),
    )
    return jax.shard_map(
        local, mesh=mesh, in_specs=in_specs, out_specs=P("ep", "tp"), check_vma=False
    )
```

```python
import jax
import jax.numpy as jnp
from jax import lax
from jax.experimental import pallas as pl
from jax.experimental.pallas import tpu as pltpu
from jax.sharding import PartitionSpec as P

F32 = jnp.float32
BF16 = jnp.bfloat16
EPS = 1e-06

X, Y, Z = 4, 4, 8
TOK = 64
HALF = 512
FULL = 1024
HID = 256
SLOTS = 8
BATCHES = 8
ROWS = 256
OTHERS = 224
PACK = 32
LAST = BATCHES - 1

NT = (((1,), (1,)), ((), ()))
TN = (((0,), (0,)), ((), ()))

ORDER = (
    "T0 X0 S0 U1", "U2 T1 T2 R1", "R2 U3 U4 S1", "S2 E0 T3 T4", "U5 U6 U7 R3", "R4 S3 S4 E1",
    "T5 T6 E2 R5", "R6 S5 S6 T7", "E3 R7 S7 C0", "E4 C1 E5 C2", "E6 C3 M0 C4", "E7 M1 M2 C5",
    "M3 C6 M4 M5", "C7 M6 M7",
)
FIRST = 0


def dot(a, b):
    return jnp.dot(a, b, preferred_element_type=F32)


def iota(shape, dim):
    return lax.broadcasted_iota(jnp.int32, shape, dim)


def rem(a, n):
    return lax.rem(a, jnp.int32(n))


def kernel(
    tok_hbm, gain_hbm, picks_hbm, pick_w_hbm, wg_hbm, wu_hbm, wd_hbm, out,
    tok, gain, picks, pick_w, wg, wu, wd, slab, meta, meta_x, meta_y, meta_in, meta_f, tri,
    gains, chosen, mixing, opening, ysend, yrecv, xsend, xrecv, msend, mrecv, fsend, frecv,
    in_sem, w_sem, w_s, w_r, g_sem, slab_r, zs, xs, mi_r, mi_s, m_r, m_s,
    y_s, y_r, x_s, x_r, p_s, p_r, f_s, f_r,
):
    ep = lax.axis_index("ep")
    c = lax.axis_index("tp")
    x = rem(ep, X)
    y = rem(ep // X, Y)
    z = ep // (X * Y)
    group = z * Y + y

    def device(xx, yy, zz, cc=c):
        return (zz * (X * Y) + yy * X + xx, cc)

    def remote(src, dst, send, recv, to):
        return pltpu.make_async_remote_copy(
            src_ref=src, dst_ref=dst, send_sem=send, recv_sem=recv,
            device_id=to, device_id_type=pl.DeviceIdType.MESH,
        )

    def along_x(d):
        return rem(x + d, X)

    def along_y(d):
        return rem(y + d, Y)

    def along_z(d):
        return rem(z + d + Z, Z)

    def core(k):
        return rem(c + k, 2)

    def offset(b):
        return (1 - 2 * (b % 2)) * ((b + 1) // 2)

    partner = (ep, 1 - c)
    barrier = pltpu.get_barrier_semaphore()

    def greet(to):
        pl.semaphore_signal(barrier, inc=1, device_id=to, device_id_type=pl.DeviceIdType.MESH)

    for d in (4, 3, 5, 2, 6, 1, 7):
        greet(device(x, y, along_z(d)))
    for d in (2, 1, 3):
        for k in range(2):
            greet(device(along_x(d), y, z, core(k)))
            greet(device(x, along_y(d), z, core(k)))
    greet(partner)

    inputs = [
        pltpu.make_async_copy(hbm, vmem, in_sem.at[i])
        for i, (hbm, vmem) in enumerate(
            ((picks_hbm, picks), (pick_w_hbm, pick_w), (tok_hbm, tok), (gain_hbm, gain))
        )
    ]
    for copy in inputs:
        copy.start()

    loads = [
        pltpu.make_async_copy(hbm.at[c], vmem.at[:, pl.ds(pl.multiple_of(c * n, n), n)], w_sem.at[i])
        for i, (hbm, vmem, n) in enumerate(((wg_hbm, wg, HID), (wu_hbm, wu, HID), (wd_hbm, wd, HALF)))
    ]
    gives = [
        remote(hbm.at[1 - c], vmem.at[:, pl.ds(pl.multiple_of(c * n, n), n)], w_s.at[0], w_r.at[0], partner)
        for i, (hbm, vmem, n) in enumerate(((wg_hbm, wg, HID), (wu_hbm, wu, HID), (wd_hbm, wd, HALF)))
    ]
    take = remote(slab.at[0:6], slab.at[0:6], w_s.at[0], w_r.at[0], partner)
    for load in loads:
        load.start()

    for copy in inputs:
        copy.wait()
    lanes = iota((TOK, ROWS), 1) - iota((TOK, ROWS), 0)
    at_x = jnp.where(lanes == x * TOK, 1.0, 0.0).astype(BF16)
    at_y = jnp.where(lanes == y * TOK, 1.0, 0.0).astype(BF16)
    names = picks[...].astype(F32).astype(BF16)
    weight = pick_w[...]
    hi = weight.astype(BF16)
    rest = weight - hi.astype(F32)
    mid = rest.astype(BF16)
    low = (rest - mid.astype(F32)).astype(BF16)
    meta_f[...] = jnp.zeros((16, ROWS), F32)
    meta_f[8:10, :] = dot(names, at_x)
    meta_x[...] = meta_f[...].astype(BF16)
    meta_f[8:10, :] = jnp.zeros((2, ROWS), F32)
    for k, part in enumerate((names, hi, mid, low)):
        meta_f[2 * k : 2 * k + 2, :] = dot(part, at_y)
    meta_y[...] = meta_f[...].astype(BF16)
    a, b = iota((ROWS, ROWS), 0), iota((ROWS, ROWS), 1)
    tri[...] = jnp.where((a // TOK == b // TOK) & (a < b), 1.0, 0.0).astype(BF16)
    slab[0, pl.ds(pl.multiple_of(x * TOK, TOK), TOK), :] = tok[...]
    gains[c] = gain[...]

    def block(b, s):
        return slab.at[b, pl.ds(pl.multiple_of(s * TOK, TOK), TOK)]

    def own_to_x(d):
        return remote(tok, block(0, x), xs.at[0], slab_r.at[0, x], device(along_x(d), y, z))

    def from_x(d):
        s = along_x(d)
        return remote(tok, block(0, s), xs.at[0], slab_r.at[0, s], device(s, y, z))

    def along(b, to, s, sign):
        return remote(
            block(b, s), block(to, s), zs.at[0], slab_r.at[to, s], device(x, y, along_z(sign))
        )

    def own_along(to, sign):
        return remote(tok, block(to, x), zs.at[0], slab_r.at[to, x], device(x, y, along_z(sign)))

    def meta_along(b, to, sign):
        return remote(meta.at[b], meta.at[to], m_s.at[0], m_r.at[to], device(x, y, along_z(sign)))

    def meta_to_x(d):
        return remote(meta_x, meta_in.at[x], mi_s.at[0], mi_r.at[0], device(along_x(d), y, z))

    def meta_to_y(d):
        return remote(meta_y, meta_in.at[X + y], mi_s.at[0], mi_r.at[0], device(x, along_y(d), z))

    meta_all = remote(meta_in.at[0:6], meta_in.at[0:6], mi_s.at[0], mi_r.at[0], partner)

    gain_give = remote(gain, gains.at[c], g_sem.at[0], g_sem.at[1], partner)
    gain_take = remote(gain, gains.at[1 - c], g_sem.at[0], g_sem.at[1], partner)

    pl.semaphore_wait(barrier, (Z - 1) + 2 * (X - 1) + 2 * (Y - 1) + 1)

    for d in (2, 1, 3):
        meta_to_x(d).start()
        meta_to_y(d).start()
    for d in (2, 1, 3):
        own_to_x(d).start()
    @pl.when(c == 0)
    def _():
        own_along(1, 1).start()
        own_along(2, -1).start()

    @pl.when(c == 1)
    def _():
        for b in range(1, BATCHES):
            own_along(b, -offset(b)).start()

    gain_give.start()

    meta_all.wait_recv()
    table = meta_x[...].astype(F32) + meta_y[...].astype(F32)
    for d in range(1, 4):
        table = table + meta_in[along_x(d)].astype(F32) + meta_in[X + along_y(d)].astype(F32)
    meta[0] = table.astype(BF16)
    meta_along(0, 1, 1).start()
    meta_along(0, 2, -1).start()

    def own_blocks():
        for d in (1, 3, 2):
            own_block(d)
        for give in gives:
            give.start()

    def own_block(d):
        from_x(d).wait_recv()

        @pl.when(c == 0)
        def _():
            s = along_x(d)
            along(0, 1, s, 1).start()
            along(0, 2, s, -1).start()

    def block_to_x(b, d):
        return remote(block(b, x), block(b, x), xs.at[0], slab_r.at[b, x], device(along_x(d), y, z))

    def tables(b):
        if b > 0:
            sign = 1 if b % 2 else -1
            meta_along(b, b, sign).wait_recv()
            if b <= 5:
                meta_along(b, b + 2, sign).start()
        prepare(b)

    def relay(b):
        sign = 1 if b % 2 else -1
        to = min(b + 2, LAST)

        @pl.when(c == 0)
        def _():
            for s in range(X):
                along(b, b, s, sign).wait_recv()
                if b <= 4 or (b == 5 and s < 2) or (b == 6 and s >= 2):
                    along(b, to, s, sign).start()

    def spread(b):
        @pl.when(c == 1)
        def _():
            along(b, b, x, 1).wait_recv()
            for d in (2, 1, 3):
                block_to_x(b, d).start()

    def gathered(b):
        if b == 0:
            return

        @pl.when(c == 1)
        def _():
            for d in (1, 3, 2):
                s = along_x(d)
                remote(block(b, s), block(b, s), xs.at[0], slab_r.at[b, s], device(s, y, z)).wait_recv()

    def part(i):
        return pl.ds(pl.multiple_of(i * PACK, PACK), PACK)

    PEERS = [(d, k) for d in (2, 1, 3, 0) for k in (0, 1) if (d, k) != (0, 0)]

    def y_message(b, d, k):
        t, j = along_y(d), core(k)
        return remote(
            ysend.at[b, part(t * 2 + j)], yrecv.at[b, part(c * Y + y)],
            y_s.at[0], y_r.at[b], device(x, t, z, j),
        )

    def y_arrival(b):
        return remote(ysend.at[b, 0:OTHERS], yrecv.at[b, 0:OTHERS], y_s.at[0], y_r.at[b], partner)

    row = iota((8, ROWS), 0)
    segment = (iota((8, ROWS), 1) // TOK).astype(F32)
    slot = iota((PACK, ROWS), 0).astype(F32)

    def spread_out(code, value):
        return jnp.concatenate(
            [jnp.where(code[q : q + 1, :] == slot, value[q : q + 1, :], 0.0) for q in range(8)], axis=0
        ).astype(BF16)

    def prepare(b):
        table = meta[b].astype(F32)
        expert = (z * 32 + row // 2 * 8 + x * 2 + rem(row, 2)).astype(F32)
        hit = jnp.where((table[8:9, :] == expert) | (table[9:10, :] == expert), 1.0, 0.0)
        member = (group * 8 + row).astype(F32)
        first, second = table[0:1, :] == member, table[1:2, :] == member
        hit_here = jnp.where(first | second, 1.0, 0.0)
        low = ((z * Y + row) * 8).astype(F32)
        hit_z = jnp.where((table[0:1, :] >= low) & (table[0:1, :] < low + 8.0) & (row < Y), 1.0, 0.0)
        ranks = dot(jnp.concatenate([hit, hit_here, hit_z, hit_z], axis=0).astype(BF16), tri[...])
        chosen[b] = spread_out(
            jnp.where(hit > 0.0, segment * SLOTS + ranks[0:8, :], -1.0), jnp.ones((8, ROWS), F32)
        )
        code = jnp.where(hit_here > 0.0, segment * SLOTS + ranks[8:16, :], -1.0)
        rank_z = jnp.where(hit_z > 0.0, ranks[16:24, :], -1.0)
        spot = jnp.sum(
            jnp.where((row == y) & (hit_z > 0.0), segment * PACK + ranks[16:24, :] + 1.0, 0.0), axis=0, keepdims=True
        )
        packing = jnp.where(spot - 1.0 == iota((Y * PACK, ROWS), 0).astype(F32), 1.0, 0.0).astype(BF16)
        for k in range(1, 4):
            value = jnp.where(first, table[2 * k : 2 * k + 1, :], 0.0) + jnp.where(
                second, table[2 * k + 1 : 2 * k + 2, :], 0.0
            )
            mixing[b, k - 1] = lax.dot_general(
                packing, spread_out(code, value), NT, preferred_element_type=F32
            ).astype(BF16)
        mine = jnp.where(iota((ROWS, TOK), 0) - iota((ROWS, TOK), 1) == y * TOK, 1.0, 0.0).astype(BF16)
        own = dot(rank_z.astype(BF16), mine)
        spots = iota((PACK, TOK), 0).astype(F32)
        opening[b] = jnp.concatenate(
            [jnp.where(own[q : q + 1, :] == spots, 1.0, 0.0) for q in range(Y)], axis=0
        ).astype(BF16)

    def select(b):
        gathered(b)
        ysend[b] = dot(chosen[b], slab[b]).astype(BF16)
        for d, k in PEERS:
            y_message(b, d, k).start()
        yrecv[b, part(c * Y + y), :] = ysend[b, part(y * 2 + c), :]

    def x_message(b, d, k):
        t, h = along_x(d), core(k)
        return remote(
            xsend.at[b, part(t * 2 + h)], xrecv.at[b, part(x * 2 + c)],
            x_s.at[0], x_r.at[b], device(t, y, z, h),
        )

    def x_arrival(b):
        return remote(xsend.at[b, 0:OTHERS], xrecv.at[b, 0:OTHERS], x_s.at[0], x_r.at[b], partner)

    def expert(b):
        y_arrival(b).wait_recv()

        if b == FIRST:
            gain_take.wait_recv()
            for load in loads:
                load.wait()
            take.wait_recv()

        low, high = yrecv[b, 0:128, :].astype(F32), yrecv[b, 128:256, :].astype(F32)
        total = jnp.sum(low * low, axis=1, keepdims=True) + jnp.sum(high * high, axis=1, keepdims=True)
        scale = lax.rsqrt(total / FULL + EPS)
        rows = jnp.concatenate(
            [(low * scale * gains[0]).astype(BF16), (high * scale * gains[1]).astype(BF16)], axis=1
        )
        gate = dot(rows, wg[...])
        up = dot(rows, wu[...])
        hidden = (gate / (1.0 + jnp.exp(-gate)) * up).astype(BF16)
        result = dot(hidden, wd[...])
        for t in range(X):
            piece = jnp.concatenate(
                [result[(s * X + t) * 8 : (s * X + t) * 8 + 8, :] for s in range(Y)], axis=0
            ).astype(BF16)
            for h in range(2):
                xsend[b, (t * 2 + h) * PACK : (t * 2 + h + 1) * PACK, :] = piece[:, h * HALF : (h + 1) * HALF]
        for d, k in PEERS:
            x_message(b, d, k).start()
        xrecv[b, part(x * 2 + c), :] = xsend[b, part(x * 2 + c), :]

    def merge_message(b, d):
        t = along_y(d)
        return remote(
            msend.at[b, part(t)], mrecv.at[b, part(y)], p_s.at[0], p_r.at[b], device(x, t, z)
        )

    def merge_arrival(b):
        return remote(msend.at[b, 0:96], mrecv.at[b, 0:96], p_s.at[0], p_r.at[b], partner)

    def combine(b):
        x_arrival(b).wait_recv()
        rows = xrecv[b]
        total = dot(mixing[b, 0], rows) + dot(mixing[b, 1], rows) + dot(mixing[b, 2], rows)
        msend[b] = total.astype(BF16)
        for d in (2, 1, 3):
            merge_message(b, d).start()
        mrecv[b, part(y), :] = msend[b, part(y), :]

    def home(b):
        return remote(fsend.at[b], frecv.at[z], f_s.at[0], f_r.at[0], device(x, y, along_z(offset(b))))

    def merge(b):
        merge_arrival(b).wait_recv()
        fsend[b] = lax.dot_general(opening[b], mrecv[b], TN, preferred_element_type=F32).astype(BF16)
        if b == 0:
            frecv[z] = fsend[0]
        else:
            home(b).start()

    stages = dict(X=lambda b: own_blocks(), T=tables, U=spread, R=relay, S=select, E=expert, C=combine, M=merge)
    for name in " ".join(ORDER).split():
        run, n = stages[name[0]], int(name[1])
        run(n)

    homes = remote(fsend.at[0 : Z - 1], frecv.at[0 : Z - 1], f_s.at[0], f_r.at[0], partner)
    homes.wait_recv()
    total = frecv[0].astype(F32)
    for i in range(1, Z):
        total = total + frecv[i].astype(F32)
    out[...] = total.astype(BF16)

    def left(send, shape_of):
        remote(shape_of, shape_of, send, f_r.at[0], partner).wait_send()

    left(mi_s.at[0], meta_in.at[0:6])
    left(m_s.at[0], meta.at[0:7])

    @pl.when(c == 0)
    def _():
        left(zs.at[0], slab.at[0:7])
        left(xs.at[0], slab.at[0, 0:192])

    @pl.when(c == 1)
    def _():
        left(zs.at[0], slab.at[0:7, 0:TOK])
        left(xs.at[0], slab.at[0:6])

    gain_give.wait_send()
    take.wait_send()
    left(y_s.at[0], ysend.at[:, 0:OTHERS])
    left(x_s.at[0], xsend.at[:, 0:OTHERS])
    left(p_s.at[0], msend.at[:, 0:96])
    homes.wait_send()


def local(tokens, norm_gain, routing, route_weight, w_gate, w_up, w_down):
    vmem = pl.BlockSpec(memory_space=pltpu.VMEM)
    hbm = pl.BlockSpec(memory_space=pltpu.HBM)
    dma = pltpu.SemaphoreType.DMA
    batch = pltpu.VMEM((BATCHES, ROWS, HALF), BF16)
    return pl.pallas_call(
        kernel,
        out_shape=jax.ShapeDtypeStruct((TOK, HALF), BF16),
        in_specs=[hbm] * 7,
        out_specs=vmem,
        scratch_shapes=[
            pltpu.VMEM((TOK, HALF), BF16),
            pltpu.VMEM((1, HALF), F32),
            pltpu.VMEM((2, TOK), jnp.int32),
            pltpu.VMEM((2, TOK), F32),
            pltpu.VMEM((FULL, 2 * HID), BF16),
            pltpu.VMEM((FULL, 2 * HID), BF16),
            pltpu.VMEM((2 * HID, FULL), BF16),
            batch,
            pltpu.VMEM((BATCHES, 16, ROWS), BF16),
            pltpu.VMEM((16, ROWS), BF16),
            pltpu.VMEM((16, ROWS), BF16),
            pltpu.VMEM((8, 16, ROWS), BF16),
            pltpu.VMEM((16, ROWS), F32),
            pltpu.VMEM((ROWS, ROWS), BF16),
            pltpu.VMEM((2, 1, HALF), F32),
            pltpu.VMEM((BATCHES, ROWS, ROWS), BF16),
            pltpu.VMEM((BATCHES, 3, Y * PACK, ROWS), BF16),
            pltpu.VMEM((BATCHES, Y * PACK, TOK), BF16),
            batch,
            batch,
            batch,
            batch,
            pltpu.VMEM((BATCHES, Y * PACK, HALF), BF16),
            pltpu.VMEM((BATCHES, Y * PACK, HALF), BF16),
            pltpu.VMEM((BATCHES, TOK, HALF), BF16),
            pltpu.VMEM((Z, TOK, HALF), BF16),
            dma((4,)),
            dma((3,)),
            dma((1,)),
            dma((1,)),
            dma((2,)),
            dma((BATCHES, X)),
            dma((1,)),
            dma((1,)),
            dma((1,)),
            dma((1,)),
            dma((BATCHES,)),
            dma((1,)),
            dma((1,)),
            dma((BATCHES,)),
            dma((1,)),
            dma((BATCHES,)),
            dma((1,)),
            dma((BATCHES,)),
            dma((1,)),
            dma((1,)),
        ],
        compiler_params=pltpu.CompilerParams(
            collective_id=0, has_side_effects=True, vmem_limit_bytes=60 << 20
        ),
    )(
        tokens, norm_gain.reshape(1, HALF), routing.T.astype(jnp.int32), route_weight.T,
        w_gate, w_up, w_down,
    )


def solution(mesh):
    in_specs = (
        P("ep", "tp"),
        P("tp"),
        P("ep", None),
        P("ep", None),
        P("ep", None, "tp"),
        P("ep", None, "tp"),
        P("ep", None, "tp"),
    )
    return jax.shard_map(
        local, mesh=mesh, in_specs=in_specs, out_specs=P("ep", "tp"), check_vma=False
    )
```
